32 devices in a mesh: ep: 8 (over z, y), tp: 4 (over x, core).
Axes of the slice: x: 2, y: 2, z: 4, core: 2. Of those that a mesh axis runs over, the one named last changes fastest.
Arguments:
- query_rows: bfloat16 [16384, 1024], P('ep', 'tp'), may hold values from -6 to 6
- key_rows: bfloat16 [16384, 1024], P('ep', 'tp'), may hold values from -6 to 6
- value_rows: bfloat16 [16384, 2048], P('ep', 'tp'), may hold values from -6 to 6
- gate_rows: bfloat16 [16384, 2048], P('ep', 'tp'), may hold values from -6 to 6
- log_decay: float32 [8, 16384], P('tp', 'ep'), may hold values from -1 to 0
- out_proj: bfloat16 [2048, 2048], P('tp'), may hold values from -0.125 to 0.125
- moe_input: bfloat16 [4096, 2048], P(('ep', 'tp')), may hold values from -6 to 6
- norm_gain: float32 [2048], replicated, may hold values from 0.1 to 1.9
- routing: int32 [4096, 4], P(('ep', 'tp')), may hold values from 0 to 31, all different within a row; in each aligned block of 128 rows (0 to 127, 128 to 255, ...) at most 32 rows name the same one
- route_weight: float32 [4096, 4], P(('ep', 'tp')), may hold values from 0.2 to 1
- expert_gate: bfloat16 [32, 2048, 512], P(('ep', 'tp')), may hold values from -0.125 to 0.125
- expert_up: bfloat16 [32, 2048, 512], P(('ep', 'tp')), may hold values from -0.125 to 0.125
- expert_down: bfloat16 [32, 512, 2048], P(('ep', 'tp')), may hold values from -0.25 to 0.25
- shared_gate: bfloat16 [2048, 512], replicated, may hold values from -0.125 to 0.125
- shared_up: bfloat16 [2048, 512], replicated, may hold values from -0.125 to 0.125
- shared_down: bfloat16 [512, 2048], replicated, may hold values from -0.25 to 0.25
Outputs:
- mixer_out: bfloat16 [16384, 2048], P(('ep', 'tp'))
- moe_out: bfloat16 [4096, 2048], P(('ep', 'tp'))
The draws below stay inside these ranges and needn't reach their ends.
Inputs may be any that keep to these rules, and one draw needn't show every extreme that they name: `routing`: within the rows of one device no expert is named more than 32 times.
All inputs are finite; a program needn't handle non-finite values.
Results may differ from the reference program's by a relative error of at most 0.019.
Values may be sent and summed in bfloat16 or wider, within the bound.
A program may use at most 128 MiB of HBM per device.

```python
import math
import jax
import jax.numpy as jnp
import numpy as np
from jax import lax

D = 2048
RETENTION_HEADS = 8
DK = 128
DV = 256
BLOCK = 128
TOK_A = 2048
TOKENS_A = 16384
FF = 512
SHARED_FF = 512
TOP = 4
TOK_B = 128
TOKENS_B = 4096
EXPERTS = 32
CAP = 32
N_EP = 8
N_TP = 4


def draw_log_decay(key, part):
    random_subkeys = jax.random.split(jax.random.fold_in(key, 17), 7)
    sequence_length = TOKENS_A
    fast_share = 0.5
    quick_decay_mask = jax.random.uniform(random_subkeys[0], (RETENTION_HEADS,)) < fast_share
    fast_rate = jnp.log(10.0) / jax.random.uniform(random_subkeys[1], (RETENTION_HEADS,), minval=30.0, maxval=100.0)
    slow_rate = jax.random.uniform(random_subkeys[2], (RETENTION_HEADS,), minval=0.2, maxval=0.6) / sequence_length
    base_rate = jnp.where(quick_decay_mask, fast_rate, slow_rate)
    position_index = jnp.arange(sequence_length)
    span_factor = jnp.exp(jax.random.uniform(random_subkeys[3], (sequence_length // TOK_A,), minval=-0.7, maxval=0.7))
    jitter = jnp.exp(jax.random.uniform(random_subkeys[4], (RETENTION_HEADS, sequence_length), minval=-0.35, maxval=0.35))
    chosen_places = jax.random.randint(random_subkeys[5], (3,), 0, sequence_length)
    spike_selected = jnp.any(position_index[None, :] == chosen_places[:, None], axis=0)
    spike_dropped = jnp.log(jax.random.uniform(random_subkeys[6], (RETENTION_HEADS, sequence_length), minval=0.5, maxval=0.8))
    smoothed_decay = -base_rate[:, None] * span_factor[position_index // TOK_A][None, :] * jitter
    selected_mask = spike_selected[None, :] & jnp.logical_not(quick_decay_mask)[:, None]
    return jnp.where(selected_mask, smoothed_decay + spike_dropped, smoothed_decay).astype(jnp.float32)


def steps_of(rng, shape, cuts, smallest, top_value):
    def one(dim, shards_of):
        steps = jax.random.uniform(jax.random.fold_in(jax.random.fold_in(rng, 6), dim), (shards_of,), jnp.float32, smallest / len(cuts), top_value / len(cuts))
        return jnp.repeat(jnp.exp(steps), shape[dim] // shards_of).reshape((-1,) + (1,) * (len(shape) - dim - 1))

    loudness = one(*cuts[0])
    for cut in cuts[1:]:
        loudness = loudness * one(*cut)
    return loudness


def deal_out(rng, own, number, rows, count, top, limit, skew):
    sequence = jax.random.permutation(rng, count)
    crowded, common = portions_of(count, rows * top, limit, skew, True), portions_of(count, rows * top, limit, skew, False)
    places = jnp.arange(count)

    def named(tallies, rotation):
        used = int((tallies > 0).sum())
        fixed = max(1, used // 4)
        passed = fixed + (places - fixed + rotation * (used - fixed)) % max(1, count - fixed)
        return jnp.zeros((count,), jnp.int32).at[sequence[jnp.where(places < fixed, places, passed)]].set(jnp.asarray(tallies, jnp.int32))

    tallies = jnp.where(number % 4 == 0, named(crowded, number // 4), named(common, number - number // 4 - 1))
    mixed = jax.random.permutation(jax.random.fold_in(own, 3), count)
    giver, taker = mixed[0:count // 2 * 2:2], mixed[1:count // 2 * 2:2]
    margin = jnp.minimum(tallies[giver] - 1, limit - tallies[taker]) // 2
    margin = jnp.where((giver == sequence[0]) | (taker == sequence[0]) | (tallies[taker] == 0), 0, jnp.maximum(margin, 0))
    passed = jax.random.randint(jax.random.fold_in(own, 4), (count // 2,), 0, 1 << 20) % (margin + 1)
    tallies = tallies.at[giver].add(-passed).at[taker].add(passed)
    items = jnp.searchsorted(jnp.cumsum(tallies), jnp.arange(rows * top), side="right").astype(jnp.int32)
    listing = items.reshape(top, rows).T
    listing = listing[jax.random.permutation(jax.random.fold_in(own, 1), rows)]
    rotation = jax.random.randint(jax.random.fold_in(own, 2), (rows, 1), 0, top)
    return jnp.take_along_axis(listing, (jnp.arange(top)[None, :] + rotation) % top, axis=1)


def portions_of(number_of, total, most, skew, full):
    portions = [(1 << 20) // math.isqrt(rank ** skew) + 1 for rank in range(1, number_of + 1)]
    largest = most if full else min(most, max(-(-total // number_of), total * portions[0] // sum(portions)))
    least = 1 if total - largest >= number_of - 1 else 0
    given, spare = [largest] + [least] * (number_of - 1), total - largest - least * (number_of - 1)
    while spare > 0:
        candidates = [i for i in range(1, number_of) if given[i] < largest] or [i for i in range(1, number_of) if given[i] < most]
        whole, budget = sum([portions[i] for i in candidates]), spare
        for i in candidates:
            more = min(most - given[i], max(1, budget * portions[i] // whole), spare)
            given[i] = given[i] + more
            spare = spare - more
    return np.array(given)


def bell_draw(rng, shape, width, reach, pieces=(), held_as=jnp.bfloat16):
    loudness = steps_of(rng, shape, pieces, -0.22, 0.18) if pieces else 1.0
    entries = jax.random.normal(rng, shape, jnp.float32) * width * loudness
    return jnp.minimum(jnp.maximum(entries, -reach), reach).astype(held_as)


def setup_inputs(seed: int = 0) -> dict:
    keys = jax.random.split(jax.random.key(seed), 17)
    query_rows = bell_draw(keys[0], (TOKENS_A, RETENTION_HEADS * DK), 1.0, 6.0, ((0, 8), (1, 4)))
    key_rows = bell_draw(keys[1], (TOKENS_A, RETENTION_HEADS * DK), 1.0, 6.0, ((0, 8), (1, 4)))
    value_rows = bell_draw(keys[2], (TOKENS_A, RETENTION_HEADS * DV), 1.0, 6.0, ((0, 8), (1, 4)))
    gate_rows = bell_draw(keys[3], (TOKENS_A, RETENTION_HEADS * DV), 1.0, 6.0, ((0, 8), (1, 4)))
    log_decay = draw_log_decay(jax.random.fold_in(keys[16], 71), 0)
    out_proj = bell_draw(keys[5], (RETENTION_HEADS * DV, D), (RETENTION_HEADS * DV) ** -0.5, 0.125, ((0, 4),))
    moe_input = bell_draw(keys[6], (TOKENS_B, D), 1.0, 6.0, ((0, 32),))
    norm_gain = jnp.clip(1.0 + 0.18 * jax.random.normal(keys[7], (D,), jnp.float32), 0.1, 1.9)
    routing_keys = jax.random.split(jax.random.fold_in(keys[8], 1), TOKENS_B // TOK_B)
    routing_turns = jax.random.permutation(jax.random.fold_in(keys[8], 3), TOKENS_B // TOK_B)
    routing = jax.vmap(lambda own, number: deal_out(jax.random.fold_in(keys[8], 2), own, number, TOK_B, EXPERTS, TOP, CAP, 2))(routing_keys, routing_turns).reshape((TOKENS_B, TOP))
    route_weight = jnp.clip(0.2 + 0.8 * jax.random.uniform(keys[9], (TOKENS_B, TOP), jnp.float32) ** steps_of(keys[9], (TOKENS_B, TOP), ((0, 32),), -0.2, 0.2), 0.2, 1.0)
    expert_gate = bell_draw(keys[10], (EXPERTS, D, FF), D ** -0.5, 0.125, ((0, 32),))
    expert_up = bell_draw(keys[11], (EXPERTS, D, FF), D ** -0.5, 0.125, ((0, 32),))
    expert_down = bell_draw(keys[12], (EXPERTS, FF, D), FF ** -0.5, 0.25, ((0, 32),))
    shared_gate = bell_draw(keys[13], (D, SHARED_FF), D ** -0.5, 0.125)
    shared_up = bell_draw(keys[14], (D, SHARED_FF), D ** -0.5, 0.125)
    shared_down = bell_draw(keys[15], (SHARED_FF, D), SHARED_FF ** -0.5, 0.25)
    return {"query_rows": query_rows, "key_rows": key_rows, "value_rows": value_rows, "gate_rows": gate_rows, "log_decay": log_decay, "out_proj": out_proj, "moe_input": moe_input, "norm_gain": norm_gain, "routing": routing, "route_weight": route_weight, "expert_gate": expert_gate, "expert_up": expert_up, "expert_down": expert_down, "shared_gate": shared_gate, "shared_up": shared_up, "shared_down": shared_down}


EPS = 1e-06

def retention_all(query_rows, key_rows, value_rows, log_decay):
    n_blocks = TOKENS_A // BLOCK
    score_scale = DK ** (-0.5)
    q_blocks = query_rows.reshape(n_blocks, BLOCK, RETENTION_HEADS, DK)
    k_blocks = key_rows.reshape(n_blocks, BLOCK, RETENTION_HEADS, DK)
    v_blocks = value_rows.reshape(n_blocks, BLOCK, RETENTION_HEADS, DV)
    a_blocks = jnp.transpose(log_decay.reshape(RETENTION_HEADS, n_blocks, BLOCK), (1, 0, 2))
    causal = jnp.arange(BLOCK)[:, None] >= jnp.arange(BLOCK)[None, :]

    def advance(carried_state, block_in):
        q_blk, k_blk, v_blk, a_blk = block_in
        cum_decay = jnp.cumsum(a_blk, axis=1)
        block_count = cum_decay[:, -1]
        query_float = q_blk.astype(jnp.float32)
        key_float = k_blk.astype(jnp.float32)
        value_float = v_blk.astype(jnp.float32)
        retention_scores = jnp.einsum('gab,lab->agl', query_float, key_float)
        log_gap = jnp.where(causal[None], cum_decay[:, :, None] - cum_decay[:, None, :], 0.0)
        decay_mat = jnp.where(causal[None], jnp.exp(log_gap), 0.0)
        weight = (retention_scores * score_scale * decay_mat).astype(jnp.bfloat16)
        weight = lax.optimization_barrier(weight).astype(jnp.float32)
        inner_out = jnp.einsum('hnm,mhe->nhe', weight, value_float)
        state_low = lax.optimization_barrier(carried_state.astype(jnp.bfloat16)).astype(jnp.float32)
        cross_out = jnp.einsum('nhd,hde->nhe', query_float, state_low) * jnp.exp(cum_decay).T[:, :, None]
        decayed_key_rows = (key_float * score_scale * jnp.exp(block_count[None, :] - cum_decay.T)[:, :, None]).astype(jnp.bfloat16)
        decayed_key_rows = lax.optimization_barrier(decayed_key_rows).astype(jnp.float32)
        carried_state = carried_state * jnp.exp(block_count)[:, None, None] + jnp.einsum('czq,czy->zqy', decayed_key_rows, value_float)
        return (carried_state, inner_out + cross_out)
    initial = jnp.zeros((RETENTION_HEADS, DK, DV), jnp.float32)
    _, outputs = lax.scan(advance, initial, (q_blocks, k_blocks, v_blocks, a_blocks))
    return outputs.reshape(TOKENS_A, RETENTION_HEADS, DV)

def expert_apply(inputs, w_gate, w_up, w_down):
    gate_act = jnp.dot(inputs, w_gate, preferred_element_type=jnp.float32)
    up_act = jnp.dot(inputs, w_up, preferred_element_type=jnp.float32)
    hidden = (jax.nn.silu(gate_act) * up_act).astype(jnp.bfloat16)
    return jnp.dot(hidden, w_down, preferred_element_type=jnp.float32)

def reference(query_rows, key_rows, value_rows, gate_rows, log_decay, out_proj, moe_input, norm_gain, routing, route_weight, expert_gate, expert_up, expert_down, shared_gate, shared_up, shared_down):
    raw_out = retention_all(query_rows, key_rows, value_rows, log_decay)
    avg_out = lax.optimization_barrier(jnp.mean(raw_out, axis=-1, keepdims=True))
    spread = lax.optimization_barrier(jnp.mean(jnp.square(raw_out - avg_out), axis=-1, keepdims=True))
    normed = (raw_out - avg_out) * lax.rsqrt(spread + EPS)
    gate_act = jax.nn.silu(gate_rows.astype(jnp.float32).reshape(TOKENS_A, RETENTION_HEADS, DV))
    retained = (gate_act * normed).reshape(TOKENS_A, RETENTION_HEADS * DV).astype(jnp.bfloat16)
    group_cols = RETENTION_HEADS * DV // N_TP
    summed = jnp.zeros((TOKENS_A, D), jnp.float32)
    for group_idx in range(N_TP):
        lo_col = group_idx * group_cols
        partial_sum = jnp.dot(retained[:, lo_col:lo_col + group_cols], out_proj[lo_col:lo_col + group_cols], preferred_element_type=jnp.float32).astype(jnp.bfloat16)
        summed = summed + partial_sum.astype(jnp.float32)
    mixer_out = summed.astype(jnp.bfloat16)
    as_float = moe_input.astype(jnp.float32)
    moe_normed = (as_float * lax.rsqrt(lax.optimization_barrier(jnp.mean(as_float * as_float, axis=-1, keepdims=True)) + EPS) * norm_gain).astype(jnp.bfloat16)
    flat_route = routing.reshape(-1)
    flat_weight = route_weight.reshape(-1)
    bound_rows = N_EP * N_TP * CAP

    def visit(total_out, expert_idx):
        picked_rows = jnp.nonzero(flat_route == expert_idx, size=bound_rows, fill_value=0)[0].astype(jnp.int32)
        live_mask = (jnp.arange(bound_rows) < jnp.sum((flat_route == expert_idx).astype(jnp.int32))).astype(jnp.float32)
        token_idx = picked_rows // TOP
        result = expert_apply(moe_normed[token_idx], expert_gate[expert_idx], expert_up[expert_idx], expert_down[expert_idx])
        result = lax.optimization_barrier(result.astype(jnp.bfloat16)).astype(jnp.float32)
        scaled = result * (flat_weight[picked_rows] * live_mask)[:, None]
        return (total_out.at[token_idx].add(scaled), None)
    routed, _ = lax.scan(visit, jnp.zeros((TOKENS_B, D), jnp.float32), jnp.arange(N_EP * N_TP, dtype=jnp.int32))
    shared = expert_apply(moe_normed, shared_gate, shared_up, shared_down)
    moe_out = (routed + shared).astype(jnp.bfloat16)
    return (mixer_out, moe_out)
```

```python
import functools
import math

import jax
import jax.numpy as jnp
from jax import lax
from jax.experimental import pallas as pl
from jax.experimental.pallas import tpu as pltpu
from jax.sharding import PartitionSpec as P

DK = 128
DV = 256
BLOCK = 128
EPS = 1e-06
Z_GROUPS = 4

F32 = jnp.float32
BF16 = jnp.bfloat16
MESH = pl.DeviceIdType.MESH


def dot(a, b):
    return jnp.dot(a, b, preferred_element_type=F32)


def silu(v):
    return v / (1.0 + jnp.exp(-v))


def kernel(
    E, T, G, C,
    gain_ref, route_ref, rweight_ref, decay_ref,
    x_hbm, q_hbm, k_hbm, v_hbm, g_hbm, op_hbm,
    wg_hbm, wu_hbm, wd_hbm, sg_hbm, su_hbm, sd_hbm,
    mix_hbm, moe_hbm,
    x_v, mix_v, moe_v, cum_ref, cumc_ref, tot_ref,
    q_v, k_v, v_v, g_v, op_v, wg_v, wu_v, wd_v,
    xz, mz, dsp, rcv, ret, dwt, shr, prcv,
    upd, sblk, lend, srcv, trcv, rs, rr, inc,
    load_sem, mix_sem, moe_sem,
    z_s, z_r, m_s, m_r, d_s, d_r, b_s, b_r, p_s, p_r, s_s, s_r, t_s, t_r,
    o1_s, o1_r, o2_s, o2_r, o3_s, o3_r, oz_s, oz_r, r_s, r_r,
):
    ep = lax.axis_index("ep")
    tp = lax.axis_index("tp")
    R = E // G
    Pn = R * T
    zi = ep // R
    yi = ep % R
    j = yi * T + tp
    tok, width = x_v.shape
    n_visits = route_ref.shape[0]
    nb = cum_ref.shape[0]
    H = cum_ref.shape[1]
    nbc = nb // T
    B = math.gcd(T, 2)
    A = T // B
    ta, tb = tp // B, tp % B
    Q = math.gcd(G, 2)
    zq = zi % Q
    piece = op_v.shape[1] // (R * Q)
    scale = DK ** (-0.5)

    loads = [
        pltpu.make_async_copy(src, dst, load_sem.at[i])
        for i, (src, dst) in enumerate(
            ((k_hbm, k_v), (v_hbm, v_v), (op_hbm, op_v.at[tp]), (sg_hbm, wg_v), (su_hbm, wu_v),
             (sd_hbm, wd_v), (q_hbm, q_v), (g_hbm, g_v), (wg_hbm.at[0], wg_v),
             (wu_hbm.at[0], wu_v), (wd_hbm.at[0], wd_v))
        )
    ]
    x_load = pltpu.make_async_copy(x_hbm, x_v, load_sem.at[11])
    x_load.start()
    for c in loads[:8]:
        c.start()

    def z_place(g):
        return (g * R + yi, tp)

    def plane_peer(d):
        p = (j + d) % Pn
        return (zi * R + p // T, p % T)

    def tp_peer(i):
        return (ep, (tp + i) % T)

    barrier = pltpu.get_barrier_semaphore()

    @pl.loop(1, Pn)
    def _(d):
        pl.semaphore_signal(barrier, inc=1, device_id=plane_peer(d), device_id_type=MESH)

    @pl.loop(1, E)
    def _(d):
        pl.semaphore_signal(barrier, inc=1, device_id=((ep + d) % E, tp), device_id_type=MESH)

    x_load.wait()
    xf = x_v[...].astype(F32)
    xz[zi] = (
        xf * lax.rsqrt(jnp.mean(xf * xf, axis=-1, keepdims=True) + EPS) * gain_ref[...]
    ).astype(BF16)
    mz[zi, 0:n_visits] = route_ref[...].astype(F32)
    mz[zi, n_visits:2 * n_visits] = rweight_ref[...]
    pl.semaphore_wait(barrier, Pn - 1 + E - 1)

    def rcopy(src, dst, ss, rs_, dev):
        return pltpu.make_async_remote_copy(
            src_ref=src, dst_ref=dst, send_sem=ss, recv_sem=rs_, device_id=dev, device_id_type=MESH
        )

    def z_copy(g, way):
        to = (zi - 1, zi + 1)[way]
        return rcopy(xz.at[g], xz.at[g], z_s.at[way, g], z_r.at[g], z_place(to))

    def m_copy(g, way):
        to = (zi - 1, zi + 1)[way]
        return rcopy(mz.at[g], mz.at[g], m_s.at[way, g], m_r.at[g], z_place(to))

    def z_sends(g, way):
        if way:
            return (g <= zi) & (zi + 1 < G)
        return (g >= zi) & (zi > 0)

    def group_at(i):
        dist = (i + 1) // 2
        g = zi + jnp.where(i % 2 == 1, -dist, dist)
        return g, (g >= 0) & (g < G)

    def rows(d):
        return pl.ds(pl.multiple_of(d * C, C), C)

    def d_copy(r, d):
        return rcopy(dsp.at[r, rows(d)], rcv.at[r, rows(d)], d_s.at[r, d], d_r.at[r, d],
                     plane_peer(d))

    def b_copy(r, d):
        return rcopy(rcv.at[r, rows(d)], ret.at[r, rows(d)], b_s.at[r, d], b_r.at[r, d],
                     plane_peer(Pn - d))

    def p_copy(g):
        return rcopy(dsp.at[g, 0:tok], prcv.at[zi], p_s.at[g], p_r.at[zi], z_place(g))

    def p_arrival(g):
        return rcopy(dsp.at[g, 0:tok], prcv.at[g], p_s.at[g], p_r.at[g], z_place(g))

    def s_copy(d):
        return rcopy(lend, srcv.at[d - 1], s_s.at[d], s_r.at[d], ((ep + d) % E, tp))

    def t_copy(d):
        return rcopy(tot_ref, trcv.at[d], t_s.at[d], t_r.at[d], ((ep + d) % E, tp))

    def shard(da, db=0):
        return ((ta + A - da) % A) * B + (tb + B - db) % B

    def part(y, q):
        return pl.ds(pl.multiple_of((q * R + y) * piece, piece), piece)

    def half(q):
        return pl.ds(pl.multiple_of(q * R * piece, R * piece), R * piece)

    def o1_copy(da, src):
        at = op_v.at[src, part(yi, zq)]
        return rcopy(at, at, o1_s.at[da], o1_r.at[da], (ep, ((ta + da) % A) * B + tb))

    def o2_copy(da, dy, y):
        at = op_v.at[shard(da), part(y, zq)]
        return rcopy(at, at, o2_s.at[da, dy], o2_r.at[da, dy], (zi * R + (yi + dy) % R, tp))

    def oz_copy(da, dz, q):
        at = op_v.at[shard(da), half(q)]
        return rcopy(at, at, oz_s.at[da, dz], oz_r.at[da, dz],
                     ((zi - zq + (zq + dz) % Q) * R + yi, tp))

    def o3_copy(da, db, src):
        at = op_v.at[src]
        return rcopy(at, at, o3_s.at[da, db], o3_r.at[da, db], (ep, ta * B + (tb + db) % B))

    def r_copy(da, db):
        i = da * B + db
        return rcopy(rs.at[i], rr.at[i - 1], r_s.at[i], r_r.at[i],
                     (ep, ((ta + da) % A) * B + (tb + db) % B))

    for way in (0, 1):
        @pl.when(z_sends(zi, way))
        def _():
            m_copy(zi, way).start()
            z_copy(zi, way).start()

    def dispatch(r):
        meta = mz[r]
        owner = lax.broadcasted_iota(jnp.int32, (Pn, tok), 0)
        owner = (zi * Pn + (owner + j) % Pn).astype(F32)
        member = jnp.zeros((Pn, tok), F32)
        weight = jnp.zeros((Pn, tok), F32)
        for v in range(n_visits):
            hit = meta[v:v + 1, :] == owner
            member += jnp.where(hit, 1.0, 0.0)
            weight += jnp.where(hit, meta[n_visits + v:n_visits + v + 1, :], 0.0)
        before = lax.broadcasted_iota(jnp.int32, (tok, tok), 0) < lax.broadcasted_iota(
            jnp.int32, (tok, tok), 1
        )
        rank = dot(member.astype(BF16), jnp.where(before, 1.0, 0.0).astype(BF16))
        rank = jnp.where(member > 0.5, rank, -1.0)
        slot = lax.broadcasted_iota(jnp.int32, (C, tok), 0).astype(F32)
        picks, wts = [], []
        for d in range(Pn):
            eq = slot == rank[d:d + 1, :]
            picks.append(jnp.where(eq, 1.0, 0.0))
            wts.append(jnp.where(eq, weight[d:d + 1, :], 0.0))
        pick = jnp.concatenate(picks, axis=0).astype(BF16)
        dwt[r] = jnp.concatenate(wts, axis=0).T.astype(BF16)
        out = dot(pick, xz[r]).astype(BF16)
        dsp[r] = out
        rcv[r, 0:C] = out[0:C]

        @pl.loop(1, Pn)
        def _(d):
            d_copy(r, d).start()

    dispatch(zi)

    blocks = jnp.concatenate(
        [decay_ref[:, b * BLOCK:(b + 1) * BLOCK] for b in range(nb)], axis=0
    )
    upto = lax.broadcasted_iota(jnp.int32, (BLOCK, BLOCK), 0) <= lax.broadcasted_iota(
        jnp.int32, (BLOCK, BLOCK), 1
    )
    cum = jnp.dot(
        blocks, jnp.where(upto, 1.0, 0.0), precision=lax.Precision.HIGHEST,
        preferred_element_type=F32,
    )
    cum_t = cum.T
    for b in range(nb):
        cum_ref[b] = cum[b * H:(b + 1) * H]
        cumc_ref[b] = cum_t[:, b * H:(b + 1) * H]
    tot_ref[...] = jnp.zeros_like(tot_ref)
    tot_ref[0:H] = jnp.broadcast_to(
        jnp.sum(decay_ref[...], axis=1, keepdims=True), (H, tot_ref.shape[1])
    )

    loads[0].wait()
    loads[1].wait()

    def state_rows(b, h):
        return pl.ds(pl.multiple_of((b * H + h) * DK, DK), DK)

    inc[...] = jnp.zeros_like(inc)

    @pl.loop(0, nb)
    def _(b):
        rb = pl.ds(pl.multiple_of(b * BLOCK, BLOCK), BLOCK)
        cumc = cumc_ref[b]
        crow = cum_ref[b]
        for h in range(H):
            col = cumc[:, h:h + 1]
            last = crow[h:h + 1, BLOCK - 1:BLOCK]
            u = (k_v[rb, h * DK:(h + 1) * DK].astype(F32) * (scale * jnp.exp(last - col))).astype(BF16)
            add = lax.dot_general(
                u, v_v[rb, h * DV:(h + 1) * DV], (((0,), (0,)), ((), ())),
                preferred_element_type=F32,
            )
            upd[state_rows(b, h)] = add
            inc[h] = inc[h] * jnp.exp(last) + add

    lend[...] = inc[...].astype(BF16)

    loads[3].wait()
    loads[4].wait()
    loads[5].wait()
    hid = (silu(dot(xz[zi], wg_v[...])) * dot(xz[zi], wu_v[...])).astype(BF16)
    shr[...] = dot(hid, wd_v[...])
    for c in loads[8:]:
        c.start()

    def serve(r):
        @pl.loop(1, Pn)
        def _(d):
            d_copy(r, d).wait_recv()

        rows_in = rcv[r]
        hidden = (silu(dot(rows_in, wg_v[...])) * dot(rows_in, wu_v[...])).astype(BF16)
        res = dot(hidden, wd_v[...]).astype(BF16)
        rcv[r] = res
        ret[r, 0:C] = res[0:C]

        @pl.loop(1, Pn)
        def _(d):
            b_copy(r, d).start()

    loads[8].wait()
    loads[9].wait()
    loads[10].wait()
    @pl.loop(1, 2 * G - 1)
    def _(i):
        g, there = group_at(i)

        @pl.when(there)
        def _():
            m_copy(g, 0).wait_recv()
            z_copy(g, 0).wait_recv()
            for way in (0, 1):
                @pl.when(z_sends(g, way))
                def _():
                    m_copy(g, way).start()
                    z_copy(g, way).start()
            dispatch(g)

        @pl.when(i == G - 1)
        def _():
            @pl.loop(1, E)
            def _(d):
                @pl.when(ep + d < E)
                def _():
                    t_copy(d).start()
                    s_copy(d).start()

        behind, known = group_at(i - 2)

        @pl.when(known & (i >= 2))
        def _():
            serve(behind)

    loads[2].wait()
    for da in range(1, A):
        o1_copy(da, tp).start()
    for i in (2 * G - 3, 2 * G - 2):
        g, there = group_at(jnp.int32(i))

        @pl.when(there)
        def _():
            serve(g)

    inc[...] = jnp.zeros_like(inc)

    @pl.loop(1, E)
    def _(i):
        d = E - i

        @pl.when(ep >= d)
        def _():
            t_copy(d).wait_recv()
            s_copy(d).wait_recv()
            for h in range(H):
                shrink = jnp.exp(trcv[d, h:h + 1, 0:1])
                inc[h] = inc[h] * shrink + srcv[d - 1, h].astype(F32)

    @pl.loop(0, nb)
    def _(b):
        crow = cum_ref[b]
        for h in range(H):
            s = inc[h]
            sblk[b, h] = s.astype(BF16)
            inc[h] = s * jnp.exp(crow[h:h + 1, BLOCK - 1:BLOCK]) + upd[state_rows(b, h)]

    loads[6].wait()
    loads[7].wait()
    causal = lax.broadcasted_iota(jnp.int32, (BLOCK, BLOCK), 0) >= lax.broadcasted_iota(
        jnp.int32, (BLOCK, BLOCK), 1
    )

    def retain(i, da, db):
        chunk = ((ta + da) % A) * B + (tb + db) % B

        @pl.loop(0, nbc)
        def _(w):
            b = chunk * nbc + w
            rb = pl.ds(pl.multiple_of(b * BLOCK, BLOCK), BLOCK)
            ro = pl.ds(pl.multiple_of(w * BLOCK, BLOCK), BLOCK)
            cumc = cumc_ref[b]
            crow = cum_ref[b]
            for h in range(H):
                col = cumc[:, h:h + 1]
                row = crow[h:h + 1, :]
                qb = q_v[rb, h * DK:(h + 1) * DK]
                kb = k_v[rb, h * DK:(h + 1) * DK]
                vb = v_v[rb, h * DV:(h + 1) * DV]
                sc = lax.dot_general(qb, kb, (((1,), (1,)), ((), ())), preferred_element_type=F32)
                dec = jnp.exp(jnp.where(causal, col - row, 0.0))
                wt = jnp.where(causal, sc * scale * dec, 0.0).astype(BF16)
                raw = dot(wt, vb) + dot(qb, sblk[b, h]) * jnp.exp(col)
                avg = jnp.mean(raw, axis=-1, keepdims=True)
                cen = raw - avg
                var = jnp.mean(cen * cen, axis=-1, keepdims=True)
                gate = g_v[rb, h * DV:(h + 1) * DV].astype(F32)
                rs[i, ro, h * DV:(h + 1) * DV] = (
                    silu(gate) * (cen * lax.rsqrt(var + EPS))
                ).astype(BF16)

    @pl.loop(1, T)
    def _(k):
        i = T - k
        retain(i, i // B, i % B)
        r_copy(i // B, i % B).start()

    retain(0, 0, 0)

    def combine(r):
        @pl.loop(1, Pn)
        def _(d):
            b_copy(r, d).wait_recv()

        @pl.loop(1, Pn)
        def _(d):
            d_copy(r, d).wait_send()

        dsp[r, 0:tok] = dot(dwt[r], ret[r]).astype(BF16)
        p_copy(r).start()

    for da in range(1, A):
        o1_copy(da, shard(da)).wait_recv()
        for dy in range(1, R):
            o2_copy(da, dy, yi).start()
    for db in range(1, B):
        o3_copy(0, db, tp).start()

    @pl.loop(1, 2 * G - 1)
    def _(i):
        g, there = group_at(i)

        @pl.when(i == G - 1)
        def _():
            for da in range(1, A):
                for dy in range(1, R):
                    o2_copy(da, dy, (yi + R - dy) % R).wait_recv()
                for dz in range(1, Q):
                    oz_copy(da, dz, zq).start()

        @pl.when(there)
        def _():
            combine(g)

    for da in range(1, A):
        for dz in range(1, Q):
            oz_copy(da, dz, (zq + Q - dz) % Q).wait_recv()
        for db in range(1, B):
            o3_copy(da, db, shard(da)).start()

    @pl.loop(1, Pn)
    def _(d):
        b_copy(zi, d).wait_recv()

    shr[...] += dot(dwt[zi], ret[zi])

    for db in range(1, B):
        o3_copy(0, db, shard(0, db)).wait_recv()
        r_copy(0, db).wait_recv()

    n_col = upd.shape[1]
    n_out = width // n_col

    def columns(n):
        return pl.ds(pl.multiple_of(n * n_col, n_col), n_col)

    def out_rows(n):
        return pl.ds(pl.multiple_of(n * mix_v.shape[0], mix_v.shape[0]), mix_v.shape[0])

    @pl.loop(0, n_out)
    def _(n):
        acc = dot(rs[0], op_v[tp, :, columns(n)])
        for db in range(1, B):
            acc += dot(rr[db - 1], op_v[shard(0, db), :, columns(n)])
        upd[out_rows(n)] = acc

    @pl.loop(1, G)
    def _(i):
        g = (zi + i) % G
        p_arrival(g).wait_recv()
        shr[...] += prcv[g].astype(F32)

    moe_v[...] = shr[...].astype(BF16)
    moe_out = pltpu.make_async_copy(moe_v, moe_hbm, moe_sem)
    moe_out.start()

    for da in range(1, A):
        for db in range(B):
            if db:
                o3_copy(da, db, shard(da, db)).wait_recv()
            r_copy(da, db).wait_recv()

    def mix_out(n):
        return pltpu.make_async_copy(
            mix_v.at[:, columns(n)], mix_hbm.at[:, columns(n)], mix_sem.at[n]
        )

    @pl.loop(0, n_out)
    def _(n):
        acc = upd[out_rows(n)]
        for da in range(1, A):
            for db in range(B):
                acc += dot(rr[da * B + db - 1], op_v[shard(da, db), :, columns(n)])
        mix_v[:, columns(n)] = acc.astype(BF16)
        mix_out(n).start()

    @pl.loop(0, G)
    def _(g):
        for way in (0, 1):
            @pl.when(z_sends(g, way))
            def _():
                m_copy(g, way).wait_send()
                z_copy(g, way).wait_send()

        @pl.when(g != zi)
        def _():
            p_copy(g).wait_send()

    @pl.loop(0, G)
    def _(r):
        @pl.loop(1, Pn)
        def _(d):
            b_copy(r, d).wait_send()

    @pl.loop(1, Pn)
    def _(d):
        d_copy(zi, d).wait_send()

    @pl.loop(1, E)
    def _(d):
        @pl.when(ep + d < E)
        def _():
            t_copy(d).wait_send()
            s_copy(d).wait_send()

    for da in range(A):
        for db in range(B):
            if da or db:
                r_copy(da, db).wait_send()

    for da in range(A):
        if da:
            o1_copy(da, tp).wait_send()
            for dy in range(1, R):
                o2_copy(da, dy, yi).wait_send()
            for dz in range(1, Q):
                oz_copy(da, dz, zq).wait_send()
        for db in range(1, B):
            o3_copy(da, db, shard(da)).wait_send()

    moe_out.wait()

    @pl.loop(0, n_out)
    def _(n):
        mix_out(n).wait()


def local(
    query_rows, key_rows, value_rows, gate_rows, log_decay, out_proj,
    moe_input, norm_gain, routing, route_weight,
    expert_gate, expert_up, expert_down, shared_gate, shared_up, shared_down,
):
    E, T = lax.axis_size("ep"), lax.axis_size("tp")
    G = math.gcd(E, Z_GROUPS)
    Pn = (E // G) * T
    n = query_rows.shape[0]
    H = query_rows.shape[1] // DK
    nb = n // BLOCK
    tok, width = moe_input.shape
    visits = routing.shape[1]
    C = 2 * tok * visits // (E * T)
    ff = expert_gate.shape[2]
    assert shared_gate.shape[1] == ff
    rows_o = n // T
    dvl = H * DV

    vm = pl.BlockSpec(memory_space=pltpu.VMEM)
    hb = pl.BlockSpec(memory_space=pl.ANY)
    V = pltpu.VMEM
    dma = pltpu.SemaphoreType.DMA
    rows_t = H + (-H % 8)
    scratch = [
        V((tok, width), BF16), V((rows_o, width), BF16), V((tok, width), BF16),
        V((nb, H, BLOCK), F32), V((nb, BLOCK, H), F32), V((rows_t, 128), F32),
        V((n, H * DK), BF16), V((n, H * DK), BF16), V((n, dvl), BF16), V((n, dvl), BF16),
        V((T,) + out_proj.shape, BF16),
        V((width, ff), BF16), V((width, ff), BF16), V((ff, width), BF16),
        V((G, tok, width), BF16), V((G, 2 * visits, tok), F32),
        V((G, Pn * C, width), BF16), V((G, Pn * C, width), BF16), V((G, Pn * C, width), BF16),
        V((G, tok, Pn * C), BF16), V((tok, width), F32), V((G, tok, width), BF16),
        V((max(nb * H * DK, rows_o * width // DV), DV), F32), V((nb, H, DK, DV), BF16), V((H, DK, DV), BF16),
        V((E - 1, H, DK, DV), BF16), V((E, rows_t, 128), F32),
        V((T, rows_o, dvl), BF16), V((T - 1, rows_o, dvl), BF16), V((H, DK, DV), F32),
        dma((12,)), dma((width // DV,)), dma,
        dma((2, G)), dma((G,)), dma((2, G)), dma((G,)),
        dma((G, Pn)), dma((G, Pn)), dma((G, Pn)), dma((G, Pn)),
        dma((G,)), dma((G,)),
        dma((E,)), dma((E,)), dma((E,)), dma((E,)),
        dma((T,)), dma((T,)), dma((T, E)), dma((T, E)), dma((T, T)), dma((T, T)),
        dma((T, G)), dma((T, G)),
        dma((T,)), dma((T,)),
    ]
    return pl.pallas_call(
        functools.partial(kernel, E, T, G, C),
        out_shape=(
            jax.ShapeDtypeStruct((rows_o, width), BF16),
            jax.ShapeDtypeStruct((tok, width), BF16),
        ),
        in_specs=[vm] * 4 + [hb] * 12,
        out_specs=(hb, hb),
        scratch_shapes=scratch,
        compiler_params=pltpu.CompilerParams(
            collective_id=0, has_side_effects=True, vmem_limit_bytes=67043328
        ),
        name="fused",
    )(
        norm_gain[None, :], routing.T, route_weight.T, log_decay,
        moe_input, query_rows, key_rows, value_rows, gate_rows, out_proj,
        expert_gate, expert_up, expert_down, shared_gate, shared_up, shared_down,
    )


def solution(mesh):
    both = P(("ep", "tp"), None)
    in_specs = (
        P("ep", "tp"), P("ep", "tp"), P("ep", "tp"), P("ep", "tp"), P("tp", "ep"), P("tp", None),
        both, P(), both, both,
        P(("ep", "tp"), None, None), P(("ep", "tp"), None, None), P(("ep", "tp"), None, None),
        P(), P(), P(),
    )
    return jax.shard_map(
        local, mesh=mesh, in_specs=in_specs, out_specs=(both, both), check_vma=False
    )
```

```python
import functools
import math

import jax
import jax.numpy as jnp
from jax import lax
from jax.experimental import pallas as pl
from jax.experimental.pallas import tpu as pltpu
from jax.sharding import PartitionSpec as P

DK = 128
DV = 256
BLOCK = 128
EPS = 1e-06
Z_GROUPS = 4

F32 = jnp.float32
BF16 = jnp.bfloat16
MESH = pl.DeviceIdType.MESH


def dot(a, b):
    return jnp.dot(a, b, preferred_element_type=F32)


def silu(v):
    return v / (1.0 + jnp.exp(-v))


def kernel(
    E, T, G, C,
    gain_ref, route_ref, rweight_ref, decay_ref,
    x_hbm, q_hbm, k_hbm, v_hbm, g_hbm, op_hbm,
    wg_hbm, wu_hbm, wd_hbm, sg_hbm, su_hbm, sd_hbm,
    mix_hbm, moe_hbm,
    x_v, mix_v, moe_v, cum_ref, cumc_ref,
    q_v, k_v, v_v, g_v, op_v, wg_v, wu_v, wd_v,
    xz, mz, dsp, rcv, ret, dwt, shr, prcv,
    upd, sblk, srcv, trcv, zrcv, ztot, pre, rs, rr, inc,
    load_sem, mix_sem, moe_sem,
    z_s, z_r, m_s, m_r, d_s, d_r, b_s, b_r, p_s, p_r, s_s, s_r, t_s, t_r, e_s, e_r, f_s, f_r,
    o1_s, o1_r, o2_s, o2_r, o3_s, o3_r, oz_s, oz_r, r_s, r_r,
):
    ep = lax.axis_index("ep")
    tp = lax.axis_index("tp")
    R = E // G
    Pn = R * T
    zi = ep // R
    yi = ep % R
    j = yi * T + tp
    tok, width = x_v.shape
    n_visits = route_ref.shape[0]
    nb = cum_ref.shape[0]
    H = cum_ref.shape[1]
    nbc = nb // T
    B = math.gcd(T, 2)
    A = T // B
    ta, tb = tp // B, tp % B
    Q = math.gcd(G, 2)
    zq = zi % Q
    piece = op_v.shape[1] // (R * Q)
    scale = DK ** (-0.5)

    loads = [
        pltpu.make_async_copy(src, dst, load_sem.at[i])
        for i, (src, dst) in enumerate(
            ((k_hbm, k_v), (v_hbm, v_v), (op_hbm, op_v.at[tp]), (sg_hbm, wg_v), (su_hbm, wu_v),
             (sd_hbm, wd_v), (q_hbm, q_v), (g_hbm, g_v), (wg_hbm.at[0], wg_v),
             (wu_hbm.at[0], wu_v), (wd_hbm.at[0], wd_v))
        )
    ]
    x_load = pltpu.make_async_copy(x_hbm, x_v, load_sem.at[11])
    x_load.start()
    for c in loads[:8]:
        c.start()

    def z_place(g):
        return (g * R + yi, tp)

    def plane_peer(d):
        p = (j + d) % Pn
        return (zi * R + p // T, p % T)

    def tp_peer(i):
        return (ep, (tp + i) % T)

    barrier = pltpu.get_barrier_semaphore()

    @pl.loop(1, Pn)
    def _(d):
        pl.semaphore_signal(barrier, inc=1, device_id=plane_peer(d), device_id_type=MESH)

    @pl.loop(1, E)
    def _(d):
        pl.semaphore_signal(barrier, inc=1, device_id=((ep + d) % E, tp), device_id_type=MESH)

    x_load.wait()
    xf = x_v[...].astype(F32)
    xz[zi] = (
        xf * lax.rsqrt(jnp.mean(xf * xf, axis=-1, keepdims=True) + EPS) * gain_ref[...]
    ).astype(BF16)
    mz[zi, 0:n_visits] = route_ref[...].astype(F32)
    mz[zi, n_visits:2 * n_visits] = rweight_ref[...]
    pl.semaphore_wait(barrier, Pn - 1 + E - 1)

    def rcopy(src, dst, ss, rs_, dev):
        return pltpu.make_async_remote_copy(
            src_ref=src, dst_ref=dst, send_sem=ss, recv_sem=rs_, device_id=dev, device_id_type=MESH
        )

    def z_copy(g, way):
        to = (zi - 1, zi + 1)[way]
        return rcopy(xz.at[g], xz.at[g], z_s.at[way, g], z_r.at[g], z_place(to))

    def m_copy(g, way):
        to = (zi - 1, zi + 1)[way]
        return rcopy(mz.at[g], mz.at[g], m_s.at[way, g], m_r.at[g], z_place(to))

    def z_sends(g, way):
        if way:
            return (g <= zi) & (zi + 1 < G)
        return (g >= zi) & (zi > 0)

    def nth(n):
        m = jnp.minimum(zi, G - 1 - zi)
        near = zi + (n // 2 if n % 2 == 0 else -((n + 1) // 2))
        far = zi + jnp.where(2 * zi > G - 1, m - n, n - m)
        return jnp.where(n <= 2 * m, near, far)

    def rows(d):
        return pl.ds(pl.multiple_of(d * C, C), C)

    def d_copy(r, d):
        return rcopy(dsp.at[r, rows(d)], rcv.at[r, rows(d)], d_s.at[r], d_r.at[r], plane_peer(d))

    def b_copy(r, d):
        return rcopy(rcv.at[r, rows(d)], ret.at[r, rows(d)], b_s.at[r], b_r.at[r],
                     plane_peer(Pn - d))

    others = pl.ds(C, (Pn - 1) * C)

    def d_all(r):
        return rcopy(dsp.at[r, others], rcv.at[r, others], d_s.at[r], d_r.at[r], plane_peer(1))

    def b_all(r):
        return rcopy(rcv.at[r, others], ret.at[r, others], b_s.at[r], b_r.at[r], plane_peer(1))

    def p_copy(g):
        return rcopy(dsp.at[g, 0:tok], prcv.at[zi], p_s.at[g], p_r.at[zi], z_place(g))

    def p_arrival(g):
        return rcopy(dsp.at[g, 0:tok], prcv.at[g], p_s.at[g], p_r.at[g], z_place(g))

    def s_copy(d):
        return rcopy(srcv.at[0], srcv.at[d], s_s.at[d], s_r.at[d],
                     (zi * R + (yi + d) % R, tp))

    def t_copy(d):
        return rcopy(trcv.at[0], trcv.at[d], t_s.at[d], t_r.at[d],
                     (zi * R + (yi + d) % R, tp))

    def e_copy(d):
        return rcopy(zrcv.at[0], zrcv.at[d], e_s.at[d], e_r.at[d], z_place((zi + d) % G))

    def f_copy(d):
        return rcopy(ztot.at[0], ztot.at[d], f_s.at[d], f_r.at[d], z_place((zi + d) % G))

    def shard(da, db=0):
        return ((ta + A - da) % A) * B + (tb + B - db) % B

    def part(y, q):
        return pl.ds(pl.multiple_of((q * R + y) * piece, piece), piece)

    def half(q):
        return pl.ds(pl.multiple_of(q * R * piece, R * piece), R * piece)

    def o1_copy(da, src):
        at = op_v.at[src, part(yi, zq)]
        return rcopy(at, at, o1_s.at[da], o1_r.at[da], (ep, ((ta + da) % A) * B + tb))

    def o2_copy(da, dy, y):
        at = op_v.at[shard(da), part(y, zq)]
        return rcopy(at, at, o2_s.at[da, dy], o2_r.at[da, dy], (zi * R + (yi + dy) % R, tp))

    def oz_copy(da, dz, q):
        at = op_v.at[shard(da), half(q)]
        return rcopy(at, at, oz_s.at[da, dz], oz_r.at[da, dz],
                     ((zi - zq + (zq + dz) % Q) * R + yi, tp))

    def o3_copy(da, db, src):
        at = op_v.at[src]
        return rcopy(at, at, o3_s.at[da, db], o3_r.at[da, db], (ep, ta * B + (tb + db) % B))

    def r_copy(da, db):
        i = da * B + db
        return rcopy(rs.at[i], rr.at[i - 1], r_s.at[i], r_r.at[i],
                     (ep, ((ta + da) % A) * B + (tb + db) % B))

    for way in (0, 1):
        @pl.when(z_sends(zi, way))
        def _():
            m_copy(zi, way).start()
            z_copy(zi, way).start()

    def dispatch(r):
        meta = mz[r]
        owner = lax.broadcasted_iota(jnp.int32, (Pn, tok), 0)
        owner = (zi * Pn + (owner + j) % Pn).astype(F32)
        member = jnp.zeros((Pn, tok), F32)
        weight = jnp.zeros((Pn, tok), F32)
        for v in range(n_visits):
            hit = meta[v:v + 1, :] == owner
            member += jnp.where(hit, 1.0, 0.0)
            weight += jnp.where(hit, meta[n_visits + v:n_visits + v + 1, :], 0.0)
        before = lax.broadcasted_iota(jnp.int32, (tok, tok), 0) < lax.broadcasted_iota(
            jnp.int32, (tok, tok), 1
        )
        rank = dot(member.astype(BF16), jnp.where(before, 1.0, 0.0).astype(BF16))
        rank = jnp.where(member > 0.5, rank, -1.0)
        slot = lax.broadcasted_iota(jnp.int32, (C, tok), 0).astype(F32)
        picks, wts = [], []
        for d in range(Pn):
            eq = slot == rank[d:d + 1, :]
            picks.append(jnp.where(eq, 1.0, 0.0))
            wts.append(jnp.where(eq, weight[d:d + 1, :], 0.0))
        pick = jnp.concatenate(picks, axis=0).astype(BF16)
        dwt[r] = jnp.concatenate(wts, axis=0).T.astype(BF16)
        out = dot(pick, xz[r]).astype(BF16)
        dsp[r] = out
        rcv[r, 0:C] = out[0:C]

        @pl.loop(1, Pn)
        def _(d):
            d_copy(r, d).start()

    dispatch(zi)

    blocks = jnp.concatenate(
        [decay_ref[:, b * BLOCK:(b + 1) * BLOCK] for b in range(nb)], axis=0
    )
    upto = lax.broadcasted_iota(jnp.int32, (BLOCK, BLOCK), 0) <= lax.broadcasted_iota(
        jnp.int32, (BLOCK, BLOCK), 1
    )
    cum = jnp.dot(
        blocks, jnp.where(upto, 1.0, 0.0), precision=lax.Precision.HIGHEST,
        preferred_element_type=F32,
    )
    cum_t = cum.T
    for b in range(nb):
        cum_ref[b] = cum[b * H:(b + 1) * H]
        cumc_ref[b] = cum_t[:, b * H:(b + 1) * H]
    trcv[0] = jnp.zeros_like(trcv[0])
    trcv[0, 0:H] = jnp.broadcast_to(
        jnp.sum(decay_ref[...], axis=1, keepdims=True), (H, trcv.shape[2])
    )

    loads[0].wait()
    loads[1].wait()

    def state_rows(b, h):
        return pl.ds(pl.multiple_of((b * H + h) * DK, DK), DK)

    inc[...] = jnp.zeros_like(inc)

    @pl.loop(0, nb)
    def _(b):
        rb = pl.ds(pl.multiple_of(b * BLOCK, BLOCK), BLOCK)
        cumc = cumc_ref[b]
        crow = cum_ref[b]
        for h in range(H):
            col = cumc[:, h:h + 1]
            last = crow[h:h + 1, BLOCK - 1:BLOCK]
            u = (k_v[rb, h * DK:(h + 1) * DK].astype(F32) * (scale * jnp.exp(last - col))).astype(BF16)
            add = lax.dot_general(
                u, v_v[rb, h * DV:(h + 1) * DV], (((0,), (0,)), ((), ())),
                preferred_element_type=F32,
            )
            upd[state_rows(b, h)] = add
            inc[h] = inc[h] * jnp.exp(last) + add

    srcv[0] = inc[...].astype(BF16)

    @pl.loop(1, R)
    def _(d):
        t_copy(d).start()
        s_copy(d).start()

    loads[3].wait()
    loads[4].wait()
    loads[5].wait()
    hid = (silu(dot(xz[zi], wg_v[...])) * dot(xz[zi], wu_v[...])).astype(BF16)
    shr[...] = dot(hid, wd_v[...])
    for c in loads[8:]:
        c.start()

    def serve(r):
        d_all(r).wait_recv()
        rows_in = rcv[r]
        hidden = (silu(dot(rows_in, wg_v[...])) * dot(rows_in, wu_v[...])).astype(BF16)
        res = dot(hidden, wd_v[...]).astype(BF16)
        rcv[r] = res
        ret[r, 0:C] = res[0:C]

        @pl.loop(1, Pn)
        def _(d):
            b_copy(r, d).start()

    def arrive(g):
        m_copy(g, 0).wait_recv()
        z_copy(g, 0).wait_recv()
        for way in (0, 1):
            @pl.when(z_sends(g, way))
            def _():
                m_copy(g, way).start()
                z_copy(g, way).start()
        dispatch(g)

    def plane_state():
        inc[...] = jnp.zeros_like(inc)
        ztot[0] = trcv[0]

        @pl.loop(1, R)
        def _(d):
            t_copy(d).wait_recv()
            s_copy(d).wait_recv()
            ztot[0] += trcv[d]

        @pl.loop(0, R)
        def _(y):
            d = (yi + R - y) % R

            @pl.when(y == yi)
            def _():
                pre[...] = inc[...]

            for h in range(H):
                inc[h] = inc[h] * jnp.exp(trcv[d, h:h + 1, 0:1]) + srcv[d, h].astype(F32)

        zrcv[0] = inc[...].astype(BF16)

        @pl.loop(1, G)
        def _(d):
            @pl.when(zi + d < G)
            def _():
                f_copy(d).start()
                e_copy(d).start()

    def carried_state():
        inc[...] = jnp.zeros_like(inc)

        @pl.loop(1, G)
        def _(i):
            d = G - i

            @pl.when(zi >= d)
            def _():
                f_copy(d).wait_recv()
                e_copy(d).wait_recv()
                for h in range(H):
                    inc[h] = inc[h] * jnp.exp(ztot[d, h:h + 1, 0:1]) + zrcv[d, h].astype(F32)

        @pl.loop(0, R)
        def _(y):
            @pl.when(y < yi)
            def _():
                for h in range(H):
                    inc[h] = inc[h] * jnp.exp(trcv[(yi + R - y) % R, h:h + 1, 0:1])

        inc[...] += pre[...]

        @pl.loop(0, nb)
        def _(b):
            crow = cum_ref[b]
            for h in range(H):
                s = inc[h]
                sblk[b, h] = s.astype(BF16)
                inc[h] = s * jnp.exp(crow[h:h + 1, BLOCK - 1:BLOCK]) + upd[state_rows(b, h)]

    causal = lax.broadcasted_iota(jnp.int32, (BLOCK, BLOCK), 0) >= lax.broadcasted_iota(
        jnp.int32, (BLOCK, BLOCK), 1
    )

    def retain(i, da, db):
        chunk = ((ta + da) % A) * B + (tb + db) % B

        @pl.loop(0, nbc)
        def _(w):
            b = chunk * nbc + w
            rb = pl.ds(pl.multiple_of(b * BLOCK, BLOCK), BLOCK)
            ro = pl.ds(pl.multiple_of(w * BLOCK, BLOCK), BLOCK)
            cumc = cumc_ref[b]
            crow = cum_ref[b]
            for h in range(H):
                col = cumc[:, h:h + 1]
                row = crow[h:h + 1, :]
                qb = q_v[rb, h * DK:(h + 1) * DK]
                kb = k_v[rb, h * DK:(h + 1) * DK]
                vb = v_v[rb, h * DV:(h + 1) * DV]
                sc = lax.dot_general(qb, kb, (((1,), (1,)), ((), ())), preferred_element_type=F32)
                dec = jnp.exp(jnp.where(causal, col - row, 0.0))
                wt = jnp.where(causal, sc * scale * dec, 0.0).astype(BF16)
                raw = dot(wt, vb) + dot(qb, sblk[b, h]) * jnp.exp(col)
                avg = jnp.mean(raw, axis=-1, keepdims=True)
                cen = raw - avg
                var = jnp.mean(cen * cen, axis=-1, keepdims=True)
                gate = g_v[rb, h * DV:(h + 1) * DV].astype(F32)
                rs[i, ro, h * DV:(h + 1) * DV] = (
                    silu(gate) * (cen * lax.rsqrt(var + EPS))
                ).astype(BF16)

    def combine(r):
        b_all(r).wait_recv()
        d_all(r).wait_send()
        dsp[r, 0:tok] = dot(dwt[r], ret[r]).astype(BF16)
        p_copy(r).start()

    near = [nth(n) for n in range(1, G)]
    for c in loads[8:]:
        c.wait()
    arrive(near[0])
    loads[2].wait()
    for da in range(1, A):
        o1_copy(da, tp).start()
    for db in range(1, B):
        o3_copy(0, db, tp).start()
    plane_state()
    arrive(near[1])
    serve(near[0])
    for da in range(1, A):
        o1_copy(da, shard(da)).wait_recv()
        for dy in range(1, R):
            o2_copy(da, dy, yi).start()
    for g in near[2:]:
        arrive(g)
    carried_state()
    loads[6].wait()
    loads[7].wait()

    @pl.loop(0, T)
    def _(i):
        retain(i, i // B, i % B)
    serve(near[1])
    for da in range(1, A):
        for dy in range(1, R):
            o2_copy(da, dy, (yi + R - dy) % R).wait_recv()
        for dz in range(1, Q):
            oz_copy(da, dz, zq).start()
    combine(near[0])
    for g in near[2:]:
        serve(g)
    serve(zi)
    for da in range(1, A):
        for db in range(B):
            r_copy(da, db).start()
    for db in range(1, B):
        r_copy(0, db).start()
    combine(near[1])
    for g in near[2:]:
        combine(g)
    for da in range(1, A):
        for dz in range(1, Q):
            oz_copy(da, dz, (zq + Q - dz) % Q).wait_recv()
        for db in range(1, B):
            o3_copy(da, db, shard(da)).start()

    b_all(zi).wait_recv()
    shr[...] += dot(dwt[zi], ret[zi])

    for db in range(1, B):
        o3_copy(0, db, shard(0, db)).wait_recv()
        r_copy(0, db).wait_recv()

    n_col = upd.shape[1]
    n_out = width // n_col

    def columns(n):
        return pl.ds(pl.multiple_of(n * n_col, n_col), n_col)

    def out_rows(n):
        return pl.ds(pl.multiple_of(n * mix_v.shape[0], mix_v.shape[0]), mix_v.shape[0])

    @pl.loop(0, n_out)
    def _(n):
        acc = dot(rs[0], op_v[tp, :, columns(n)])
        for db in range(1, B):
            acc += dot(rr[db - 1], op_v[shard(0, db), :, columns(n)])
        upd[out_rows(n)] = acc

    @pl.loop(1, G)
    def _(i):
        g = (zi + i) % G
        p_arrival(g).wait_recv()
        shr[...] += prcv[g].astype(F32)

    moe_v[...] = shr[...].astype(BF16)
    moe_out = pltpu.make_async_copy(moe_v, moe_hbm, moe_sem)
    moe_out.start()

    def mix_out(n):
        return pltpu.make_async_copy(
            mix_v.at[:, columns(n)], mix_hbm.at[:, columns(n)], mix_sem.at[n]
        )

    for da in range(1, A):
        for db in range(B):
            if db:
                o3_copy(da, db, shard(da, db)).wait_recv()
            r_copy(da, db).wait_recv()

            @pl.loop(0, n_out)
            def _(n):
                acc = upd[out_rows(n)] + dot(
                    rr[da * B + db - 1], op_v[shard(da, db), :, columns(n)]
                )
                if da == A - 1 and db == B - 1:
                    mix_v[:, columns(n)] = acc.astype(BF16)
                    mix_out(n).start()
                else:
                    upd[out_rows(n)] = acc

    @pl.loop(0, G)
    def _(g):
        for way in (0, 1):
            @pl.when(z_sends(g, way))
            def _():
                m_copy(g, way).wait_send()
                z_copy(g, way).wait_send()

        @pl.when(g != zi)
        def _():
            p_copy(g).wait_send()

    @pl.loop(0, G)
    def _(r):
        b_all(r).wait_send()

    d_all(zi).wait_send()

    @pl.loop(1, R)
    def _(d):
        t_copy(d).wait_send()
        s_copy(d).wait_send()

    @pl.loop(1, G)
    def _(d):
        @pl.when(zi + d < G)
        def _():
            f_copy(d).wait_send()
            e_copy(d).wait_send()

    for da in range(A):
        for db in range(B):
            if da or db:
                r_copy(da, db).wait_send()

    for da in range(A):
        if da:
            o1_copy(da, tp).wait_send()
            for dy in range(1, R):
                o2_copy(da, dy, yi).wait_send()
            for dz in range(1, Q):
                oz_copy(da, dz, zq).wait_send()
        for db in range(1, B):
            o3_copy(da, db, shard(da)).wait_send()

    moe_out.wait()

    @pl.loop(0, n_out)
    def _(n):
        mix_out(n).wait()


def local(
    query_rows, key_rows, value_rows, gate_rows, log_decay, out_proj,
    moe_input, norm_gain, routing, route_weight,
    expert_gate, expert_up, expert_down, shared_gate, shared_up, shared_down,
):
    E, T = lax.axis_size("ep"), lax.axis_size("tp")
    G = math.gcd(E, Z_GROUPS)
    R = E // G
    Pn = R * T
    B = math.gcd(T, 2)
    A = T // B
    Q = math.gcd(G, 2)
    n = query_rows.shape[0]
    H = query_rows.shape[1] // DK
    nb = n // BLOCK
    tok, width = moe_input.shape
    visits = routing.shape[1]
    C = 2 * tok * visits // (E * T)
    ff = expert_gate.shape[2]
    assert shared_gate.shape[1] == ff
    rows_o = n // T
    dvl = H * DV

    vm = pl.BlockSpec(memory_space=pltpu.VMEM)
    hb = pl.BlockSpec(memory_space=pl.ANY)
    V = pltpu.VMEM
    dma = pltpu.SemaphoreType.DMA
    rows_t = H + (-H % 8)
    scratch = [
        V((tok, width), BF16), V((rows_o, width), BF16), V((tok, width), BF16),
        V((nb, H, BLOCK), F32), V((nb, BLOCK, H), F32),
        V((n, H * DK), BF16), V((n, H * DK), BF16), V((n, dvl), BF16), V((n, dvl), BF16),
        V((T,) + out_proj.shape, BF16),
        V((width, ff), BF16), V((width, ff), BF16), V((ff, width), BF16),
        V((G, tok, width), BF16), V((G, 2 * visits, tok), F32),
        V((G, Pn * C, width), BF16), V((G, Pn * C, width), BF16), V((G, Pn * C, width), BF16),
        V((G, tok, Pn * C), BF16), V((tok, width), F32), V((G, tok, width), BF16),
        V((max(nb * H * DK, rows_o * width // DV), DV), F32), V((nb, H, DK, DV), BF16),
        V((R, H, DK, DV), BF16), V((R, rows_t, 128), F32),
        V((G, H, DK, DV), BF16), V((G, rows_t, 128), F32), V((H, DK, DV), F32),
        V((T, rows_o, dvl), BF16), V((T - 1, rows_o, dvl), BF16), V((H, DK, DV), F32),
        dma((12,)), dma((width // DV,)), dma,
        dma((2, G)), dma((G,)), dma((2, G)), dma((G,)),
        dma((G,)), dma((G,)), dma((G,)), dma((G,)),
        dma((G,)), dma((G,)),
        dma((R,)), dma((R,)), dma((R,)), dma((R,)), dma((G,)), dma((G,)), dma((G,)), dma((G,)),
        dma((A,)), dma((A,)), dma((A, R)), dma((A, R)), dma((A, B)), dma((A, B)),
        dma((A, Q)), dma((A, Q)), dma((T,)), dma((T,)),
    ]
    return pl.pallas_call(
        functools.partial(kernel, E, T, G, C),
        out_shape=(
            jax.ShapeDtypeStruct((rows_o, width), BF16),
            jax.ShapeDtypeStruct((tok, width), BF16),
        ),
        in_specs=[vm] * 4 + [hb] * 12,
        out_specs=(hb, hb),
        scratch_shapes=scratch,
        compiler_params=pltpu.CompilerParams(
            collective_id=0, has_side_effects=True, vmem_limit_bytes=67043328
        ),
        name="fused",
    )(
        norm_gain[None, :], routing.T, route_weight.T, log_decay,
        moe_input, query_rows, key_rows, value_rows, gate_rows, out_proj,
        expert_gate, expert_up, expert_down, shared_gate, shared_up, shared_down,
    )


def solution(mesh):
    both = P(("ep", "tp"), None)
    in_specs = (
        P("ep", "tp"), P("ep", "tp"), P("ep", "tp"), P("ep", "tp"), P("tp", "ep"), P("tp", None),
        both, P(), both, both,
        P(("ep", "tp"), None, None), P(("ep", "tp"), None, None), P(("ep", "tp"), None, None),
        P(), P(), P(),
    )
    return jax.shard_map(
        local, mesh=mesh, in_specs=in_specs, out_specs=(both, both), check_vma=False
    )
```

```python
import functools
import math

import jax
import jax.numpy as jnp
from jax import lax
from jax.experimental import pallas as pl
from jax.experimental.pallas import tpu as pltpu
from jax.sharding import PartitionSpec as P

DK = 128
DV = 256
BLOCK = 128
EPS = 1e-06
Z_GROUPS = 4

F32 = jnp.float32
BF16 = jnp.bfloat16
MESH = pl.DeviceIdType.MESH


def dot(a, b):
    return jnp.dot(a, b, preferred_element_type=F32)


def silu(v):
    return v / (1.0 + jnp.exp(-v))


def kernel(
    E, T, G, C,
    gain_ref, route_ref, rweight_ref, decay_ref,
    x_hbm, q_hbm, k_hbm, v_hbm, g_hbm, op_hbm,
    wg_hbm, wu_hbm, wd_hbm, sg_hbm, su_hbm, sd_hbm,
    mix_hbm, moe_hbm,
    x_v, mix_v, moe_v, cum_ref, cumc_ref,
    q_v, k_v, v_v, g_v, op_v, wg_v, wu_v, wd_v,
    xz, mz, dsp, rcv, ret, dwt, shr, prcv,
    upd, sblk, srcv, trcv, zrcv, ztot, pre, rs, rr, inc,
    load_sem, mix_sem, moe_sem,
    z_s, z_r, m_s, m_r, d_s, d_r, b_s, b_r, p_s, p_r, s_s, s_r, t_s, t_r, e_s, e_r, f_s, f_r,
    o1_s, o1_r, o2_s, o2_r, o3_s, o3_r, oz_s, oz_r, r_s, r_r,
):
    ep = lax.axis_index("ep")
    tp = lax.axis_index("tp")
    R = E // G
    Pn = R * T
    zi = ep // R
    yi = ep % R
    j = yi * T + tp
    tok, width = x_v.shape
    n_visits = route_ref.shape[0]
    nb = cum_ref.shape[0]
    H = cum_ref.shape[1]
    nbc = nb // T
    B = math.gcd(T, 2)
    A = T // B
    ta, tb = tp // B, tp % B
    piece = op_v.shape[1] // E
    scale = DK ** (-0.5)

    loads = [
        pltpu.make_async_copy(src, dst, load_sem.at[i])
        for i, (src, dst) in enumerate(
            ((k_hbm, k_v), (v_hbm, v_v), (op_hbm, op_v.at[tp]), (sg_hbm, wg_v), (su_hbm, wu_v),
             (sd_hbm, wd_v), (q_hbm, q_v), (g_hbm, g_v), (wg_hbm.at[0], wg_v),
             (wu_hbm.at[0], wu_v), (wd_hbm.at[0], wd_v))
        )
    ]
    x_load = pltpu.make_async_copy(x_hbm, x_v, load_sem.at[11])
    x_load.start()
    for c in loads[:8]:
        c.start()

    def z_place(g):
        return (g * R + yi, tp)

    def plane_peer(d):
        p = (j + d) % Pn
        return (zi * R + p // T, p % T)

    barrier = pltpu.get_barrier_semaphore()

    @pl.loop(1, Pn)
    def _(d):
        pl.semaphore_signal(barrier, inc=1, device_id=plane_peer(d), device_id_type=MESH)

    @pl.loop(1, E)
    def _(d):
        pl.semaphore_signal(barrier, inc=1, device_id=((ep + d) % E, tp), device_id_type=MESH)

    x_load.wait()
    xf = x_v[...].astype(F32)
    xz[zi] = (
        xf * lax.rsqrt(jnp.mean(xf * xf, axis=-1, keepdims=True) + EPS) * gain_ref[...]
    ).astype(BF16)
    mz[zi, 0:n_visits] = route_ref[...].astype(F32)
    mz[zi, n_visits:2 * n_visits] = rweight_ref[...]
    pl.semaphore_wait(barrier, Pn - 1 + E - 1)

    def rcopy(src, dst, ss, rs_, dev):
        return pltpu.make_async_remote_copy(
            src_ref=src, dst_ref=dst, send_sem=ss, recv_sem=rs_, device_id=dev, device_id_type=MESH
        )

    def z_copy(g, way):
        to = (zi - 1, zi + 1)[way]
        return rcopy(xz.at[g], xz.at[g], z_s.at[way, g], z_r.at[g], z_place(to))

    def m_copy(g, way):
        to = (zi - 1, zi + 1)[way]
        return rcopy(mz.at[g], mz.at[g], m_s.at[way, g], m_r.at[g], z_place(to))

    def z_sends(g, way):
        if way:
            return (g <= zi) & (zi + 1 < G)
        return (g >= zi) & (zi > 0)

    def nth(n):
        m = jnp.minimum(zi, G - 1 - zi)
        step = (2 * (zi % 2) - 1) * (2 * (n % 2) - 1)
        far = zi + jnp.where(2 * zi > G - 1, m - n, n - m)
        return jnp.where(n <= 2 * m, zi + step * ((n + 1) // 2), far)

    def rows(d):
        return pl.ds(pl.multiple_of(d * C, C), C)

    def d_copy(r, d):
        return rcopy(dsp.at[r, rows(d)], rcv.at[r, rows(d)], d_s.at[r], d_r.at[r], plane_peer(d))

    def b_copy(r, d):
        return rcopy(rcv.at[r, rows(d)], ret.at[r, rows(d)], b_s.at[r], b_r.at[r],
                     plane_peer(Pn - d))

    others = pl.ds(C, (Pn - 1) * C)

    def d_all(r):
        return rcopy(dsp.at[r, others], rcv.at[r, others], d_s.at[r], d_r.at[r], plane_peer(1))

    def b_all(r):
        return rcopy(rcv.at[r, others], ret.at[r, others], b_s.at[r], b_r.at[r], plane_peer(1))

    def p_copy(g):
        return rcopy(dsp.at[g, 0:tok], prcv.at[zi], p_s.at[g], p_r.at[zi], z_place(g))

    def p_arrival(g):
        return rcopy(dsp.at[g, 0:tok], prcv.at[g], p_s.at[g], p_r.at[g], z_place(g))

    def s_copy(d):
        return rcopy(srcv.at[0], srcv.at[d], s_s.at[d], s_r.at[d],
                     (zi * R + (yi + d) % R, tp))

    def t_copy(d):
        return rcopy(trcv.at[0], trcv.at[d], t_s.at[d], t_r.at[d],
                     (zi * R + (yi + d) % R, tp))

    def e_copy(d):
        return rcopy(zrcv.at[0], zrcv.at[d], e_s.at[d], e_r.at[d], z_place((zi + d) % G))

    def f_copy(d):
        return rcopy(ztot.at[0], ztot.at[d], f_s.at[d], f_r.at[d], z_place((zi + d) % G))

    def shard(da, db=0):
        return ((ta + A - da) % A) * B + (tb + B - db) % B

    def part(y):
        return pl.ds(pl.multiple_of((zi * R + y) * piece, piece), piece)

    def o1_copy(da, src):
        at = op_v.at[src, part(yi)]
        return rcopy(at, at, o1_s.at[da], o1_r.at[da], (ep, ((ta + da) % A) * B + tb))

    def o2_copy(da, dy, y):
        at = op_v.at[shard(da), part(y)]
        return rcopy(at, at, o2_s.at[da, dy], o2_r.at[da, dy], (zi * R + (yi + dy) % R, tp))

    def oz_copy(da, g, way):
        to = (zi - 1, zi + 1)[way]
        at = op_v.at[shard(da), pl.ds(pl.multiple_of(g * R * piece, R * piece), R * piece)]
        return rcopy(at, at, oz_s.at[da, way, g], oz_r.at[da, g], z_place(to))

    def oz_sends(g):
        for da in range(1, A):
            for way in (0, 1):
                @pl.when(z_sends(g, way))
                def _():
                    oz_copy(da, g, way).start()

    def oz_receive(g):
        for da in range(1, A):
            oz_copy(da, g, 0).wait_recv()
        oz_sends(g)

    def o3_copy(da, db, src):
        at = op_v.at[src]
        return rcopy(at, at, o3_s.at[da, db], o3_r.at[da, db], (ep, ta * B + (tb + db) % B))

    halves = 1
    strip = mix_v.shape[0] // halves

    def strip_of(part):
        return slice(part * strip, (part + 1) * strip)

    def r_copy(da, db, part):
        i = da * B + db
        return rcopy(rs.at[i, strip_of(w)], rr.at[i - 1, strip_of(w)],
                     r_s.at[i, part], r_r.at[i, part],
                     (ep, ((ta + da) % A) * B + (tb + db) % B))

    for way in (0, 1):
        @pl.when(z_sends(zi, way))
        def _():
            m_copy(zi, way).start()
            z_copy(zi, way).start()

    def dispatch(r):
        meta = mz[r]
        owner = lax.broadcasted_iota(jnp.int32, (Pn, tok), 0)
        owner = (zi * Pn + (owner + j) % Pn).astype(F32)
        member = jnp.zeros((Pn, tok), F32)
        weight = jnp.zeros((Pn, tok), F32)
        for v in range(n_visits):
            hit = meta[v:v + 1, :] == owner
            member += jnp.where(hit, 1.0, 0.0)
            weight += jnp.where(hit, meta[n_visits + v:n_visits + v + 1, :], 0.0)
        before = lax.broadcasted_iota(jnp.int32, (tok, tok), 0) < lax.broadcasted_iota(
            jnp.int32, (tok, tok), 1
        )
        rank = dot(member.astype(BF16), jnp.where(before, 1.0, 0.0).astype(BF16))
        rank = jnp.where(member > 0.5, rank, -1.0)
        slot = lax.broadcasted_iota(jnp.int32, (C, tok), 0).astype(F32)
        picks, wts = [], []
        for d in range(Pn):
            eq = slot == rank[d:d + 1, :]
            picks.append(jnp.where(eq, 1.0, 0.0))
            wts.append(jnp.where(eq, weight[d:d + 1, :], 0.0))
        pick = jnp.concatenate(picks, axis=0).astype(BF16)
        dwt[r] = jnp.concatenate(wts, axis=0).T.astype(BF16)
        out = dot(pick, xz[r]).astype(BF16)
        dsp[r] = out
        rcv[r, 0:C] = out[0:C]

        @pl.loop(1, Pn)
        def _(d):
            d_copy(r, d).start()

    loads[2].wait()
    for da in range(1, A):
        o1_copy(da, tp).start()

    dispatch(zi)

    blocks = jnp.concatenate(
        [decay_ref[:, b * BLOCK:(b + 1) * BLOCK] for b in range(nb)], axis=0
    )
    upto = lax.broadcasted_iota(jnp.int32, (BLOCK, BLOCK), 0) <= lax.broadcasted_iota(
        jnp.int32, (BLOCK, BLOCK), 1
    )
    cum = jnp.dot(
        blocks, jnp.where(upto, 1.0, 0.0), precision=lax.Precision.HIGHEST,
        preferred_element_type=F32,
    )
    cum_t = cum.T
    for b in range(nb):
        cum_ref[b] = cum[b * H:(b + 1) * H]
        cumc_ref[b] = cum_t[:, b * H:(b + 1) * H]
    trcv[0] = jnp.zeros_like(trcv[0])
    trcv[0, 0:H] = jnp.broadcast_to(
        jnp.sum(decay_ref[...], axis=1, keepdims=True), (H, trcv.shape[2])
    )

    loads[0].wait()
    loads[1].wait()

    def state_rows(b, h):
        return pl.ds(pl.multiple_of((b * H + h) * DK, DK), DK)

    inc[...] = jnp.zeros_like(inc)

    @pl.loop(0, nb)
    def _(b):
        rb = pl.ds(pl.multiple_of(b * BLOCK, BLOCK), BLOCK)
        cumc = cumc_ref[b]
        crow = cum_ref[b]
        for h in range(H):
            col = cumc[:, h:h + 1]
            last = crow[h:h + 1, BLOCK - 1:BLOCK]
            u = (k_v[rb, h * DK:(h + 1) * DK].astype(F32) * (scale * jnp.exp(last - col))).astype(BF16)
            add = lax.dot_general(
                u, v_v[rb, h * DV:(h + 1) * DV], (((0,), (0,)), ((), ())),
                preferred_element_type=F32,
            )
            upd[state_rows(b, h)] = add
            inc[h] = inc[h] * jnp.exp(last) + add

    srcv[0] = inc[...].astype(BF16)

    @pl.loop(1, R)
    def _(d):
        t_copy(d).start()
        s_copy(d).start()

    loads[3].wait()
    loads[4].wait()
    loads[5].wait()
    hid = (silu(dot(xz[zi], wg_v[...])) * dot(xz[zi], wu_v[...])).astype(BF16)
    shr[...] = dot(hid, wd_v[...])
    for c in loads[8:]:
        c.start()

    def serve(r):
        d_all(r).wait_recv()
        rows_in = rcv[r]
        hidden = (silu(dot(rows_in, wg_v[...])) * dot(rows_in, wu_v[...])).astype(BF16)
        res = dot(hidden, wd_v[...]).astype(BF16)
        rcv[r] = res
        ret[r, 0:C] = res[0:C]

        @pl.loop(1, Pn)
        def _(d):
            b_copy(r, d).start()

    def receive(g):
        m_copy(g, 0).wait_recv()
        z_copy(g, 0).wait_recv()
        for way in (0, 1):
            @pl.when(z_sends(g, way))
            def _():
                m_copy(g, way).start()
                z_copy(g, way).start()

    def plane_state():
        inc[...] = jnp.zeros_like(inc)
        ztot[0] = trcv[0]

        @pl.loop(1, R)
        def _(d):
            t_copy(d).wait_recv()
            s_copy(d).wait_recv()
            ztot[0] += trcv[d]

        @pl.loop(0, R)
        def _(y):
            d = (yi + R - y) % R

            @pl.when(y == yi)
            def _():
                pre[...] = inc[...]

            for h in range(H):
                inc[h] = inc[h] * jnp.exp(trcv[d, h:h + 1, 0:1]) + srcv[d, h].astype(F32)

        zrcv[0] = inc[...].astype(BF16)

        @pl.loop(1, G)
        def _(d):
            @pl.when(zi + d < G)
            def _():
                f_copy(d).start()
                e_copy(d).start()

    def carried_state():
        inc[...] = jnp.zeros_like(inc)

        @pl.loop(1, G)
        def _(i):
            d = G - i

            @pl.when(zi >= d)
            def _():
                f_copy(d).wait_recv()
                e_copy(d).wait_recv()
                for h in range(H):
                    inc[h] = inc[h] * jnp.exp(ztot[d, h:h + 1, 0:1]) + zrcv[d, h].astype(F32)

        @pl.loop(0, R)
        def _(y):
            @pl.when(y < yi)
            def _():
                for h in range(H):
                    inc[h] = inc[h] * jnp.exp(trcv[(yi + R - y) % R, h:h + 1, 0:1])

        inc[...] += pre[...]

        @pl.loop(0, nb)
        def _(b):
            crow = cum_ref[b]
            for h in range(H):
                s = inc[h]
                sblk[b, h] = s.astype(BF16)
                inc[h] = s * jnp.exp(crow[h:h + 1, BLOCK - 1:BLOCK]) + upd[state_rows(b, h)]

    causal = lax.broadcasted_iota(jnp.int32, (BLOCK, BLOCK), 0) >= lax.broadcasted_iota(
        jnp.int32, (BLOCK, BLOCK), 1
    )

    def retain(i, da, db):
        chunk = ((ta + da) % A) * B + (tb + db) % B

        @pl.loop(0, nbc)
        def _(w):
            b = chunk * nbc + w
            rb = pl.ds(pl.multiple_of(b * BLOCK, BLOCK), BLOCK)
            ro = pl.ds(pl.multiple_of(w * BLOCK, BLOCK), BLOCK)
            cumc = cumc_ref[b]
            crow = cum_ref[b]
            for h in range(H):
                col = cumc[:, h:h + 1]
                row = crow[h:h + 1, :]
                qb = q_v[rb, h * DK:(h + 1) * DK]
                kb = k_v[rb, h * DK:(h + 1) * DK]
                vb = v_v[rb, h * DV:(h + 1) * DV]
                sc = lax.dot_general(qb, kb, (((1,), (1,)), ((), ())), preferred_element_type=F32)
                dec = jnp.exp(jnp.where(causal, col - row, 0.0))
                wt = jnp.where(causal, sc * scale * dec, 0.0).astype(BF16)
                raw = dot(wt, vb) + dot(qb, sblk[b, h]) * jnp.exp(col)
                avg = jnp.mean(raw, axis=-1, keepdims=True)
                cen = raw - avg
                var = jnp.mean(cen * cen, axis=-1, keepdims=True)
                gate = g_v[rb, h * DV:(h + 1) * DV].astype(F32)
                rs[i, ro, h * DV:(h + 1) * DV] = (
                    silu(gate) * (cen * lax.rsqrt(var + EPS))
                ).astype(BF16)

    def combine(r):
        b_all(r).wait_recv()
        d_all(r).wait_send()
        dsp[r, 0:tok] = dot(dwt[r], ret[r]).astype(BF16)
        p_copy(r).start()

    near = [nth(n) for n in range(1, G)]
    for c in loads[8:]:
        c.wait()
    edge = (zi == 0) | (zi == G - 1)
    for da in range(1, A):
        o1_copy(da, shard(da)).wait_recv()
        for dy in range(1, R):
            o2_copy(da, dy, yi).start()
    for db in range(1, B):
        o3_copy(0, db, tp).start()
    receive(near[0])

    @pl.when(jnp.logical_not(edge))
    def _():
        receive(near[1])

    dispatch(near[0])
    plane_state()

    @pl.when(edge)
    def _():
        receive(near[1])

    dispatch(near[1])
    @pl.when(jnp.logical_not(edge))
    def _():
        for g in near[2:]:
            receive(g)
    serve(near[0])
    @pl.when(edge)
    def _():
        for g in near[2:]:
            receive(g)

    for g in near[2:]:
        dispatch(g)
    for da in range(1, A):
        for dy in range(1, R):
            o2_copy(da, dy, (yi + R - dy) % R).wait_recv()
    oz_sends(zi)
    serve(near[1])
    oz_receive(near[0])
    combine(near[0])
    oz_receive(near[1])
    @pl.when(jnp.logical_not(edge))
    def _():
        for g in near[2:]:
            oz_receive(g)
    for g in near[2:]:
        serve(g)
    carried_state()
    loads[6].wait()
    loads[7].wait()

    @pl.loop(0, T)
    def _(i):
        retain(i, i // B, i % B)
    for w in range(halves):
        for da in range(1, A):
            for db in range(B):
                r_copy(da, db, w).start()
        for db in range(1, B):
            r_copy(0, db, w).start()
    serve(zi)
    combine(near[1])
    for g in near[2:]:
        combine(g)
    @pl.when(edge)
    def _():
        for g in near[2:]:
            oz_receive(g)
    for da in range(1, A):
        for db in range(1, B):
            o3_copy(da, db, shard(da)).start()

    for db in range(1, B):
        o3_copy(0, db, shard(0, db)).wait_recv()
        for w in range(halves):
            r_copy(0, db, w).wait_recv()

    n_half = upd.shape[1]
    n_col = 2 * n_half
    n_out = width // n_col

    def columns(n):
        return pl.ds(pl.multiple_of(n * n_col, n_col), n_col)

    def out_rows(n, part):
        return pl.ds(pl.multiple_of((n * 2 + part) * strip, strip), strip)

    @pl.loop(0, n_out)
    def _(n):
        acc = dot(rs[0], op_v[tp, :, columns(n)])
        for db in range(1, B):
            acc += dot(rr[db - 1], op_v[shard(0, db), :, columns(n)])
        for w in range(2):
            upd[out_rows(n, w)] = acc[:, w * n_half:(w + 1) * n_half]

    def mix_out(n, part):
        at = (strip_of(part), columns(n))
        return pltpu.make_async_copy(mix_v.at[at], mix_hbm.at[at], mix_sem.at[n, part])

    for w in range(halves):
        for da in range(1, A):
            for db in range(B):
                if db and not w:
                    o3_copy(da, db, shard(da, db)).wait_recv()
                r_copy(da, db, w).wait_recv()

                @pl.loop(0, n_out)
                def _(n):
                    acc = dot(rr[da * B + db - 1], op_v[shard(da, db), :, columns(n)])
                    for w in range(2):
                        at = slice(w * n_half, (w + 1) * n_half)
                        part_sum = upd[out_rows(n, w)] + acc[:, at]
                        if da == A - 1 and db == B - 1:
                            mix_v[:, pl.ds(pl.multiple_of(n * n_col + w * n_half, n_half), n_half)] = (
                                part_sum.astype(BF16)
                            )
                        else:
                            upd[out_rows(n, w)] = part_sum
                    if da == A - 1 and db == B - 1:
                        mix_out(n, 0).start()

    b_all(zi).wait_recv()
    shr[...] += dot(dwt[zi], ret[zi])
    @pl.loop(1, G)
    def _(i):
        g = (zi + i) % G
        p_arrival(g).wait_recv()
        shr[...] += prcv[g].astype(F32)

    moe_v[...] = shr[...].astype(BF16)
    moe_out = pltpu.make_async_copy(moe_v, moe_hbm, moe_sem)
    moe_out.start()

    @pl.loop(0, G)
    def _(g):
        for way in (0, 1):
            @pl.when(z_sends(g, way))
            def _():
                m_copy(g, way).wait_send()
                z_copy(g, way).wait_send()

        @pl.when(g != zi)
        def _():
            p_copy(g).wait_send()

    @pl.loop(0, G)
    def _(r):
        b_all(r).wait_send()

    d_all(zi).wait_send()

    @pl.loop(1, R)
    def _(d):
        t_copy(d).wait_send()
        s_copy(d).wait_send()

    @pl.loop(1, G)
    def _(d):
        @pl.when(zi + d < G)
        def _():
            f_copy(d).wait_send()
            e_copy(d).wait_send()

    for da in range(A):
        for db in range(B):
            if da or db:
                for w in range(halves):
                    r_copy(da, db, w).wait_send()

    for da in range(A):
        if da:
            o1_copy(da, tp).wait_send()
            for dy in range(1, R):
                o2_copy(da, dy, yi).wait_send()
            for g in range(G):
                for way in (0, 1):
                    @pl.when(z_sends(g, way))
                    def _():
                        oz_copy(da, g, way).wait_send()
        for db in range(1, B):
            o3_copy(da, db, shard(da)).wait_send()

    moe_out.wait()

    @pl.loop(0, n_out)
    def _(n):
        for w in range(halves):
            mix_out(n, w).wait()


def finish(mix_in, moe_in, mix_out, moe_out, mix_v, moe_v, in_sem, out_sem):
    parts = in_sem.shape[0] - 1
    strip = mix_v.shape[0] // parts

    def pair(i):
        if i == parts:
            refs = (moe_in, moe_v, moe_out)
        else:
            refs = [r.at[i * strip:(i + 1) * strip] for r in (mix_in, mix_v, mix_out)]
        return (pltpu.make_async_copy(refs[0], refs[1], in_sem.at[i]),
                pltpu.make_async_copy(refs[1], refs[2], out_sem.at[i]))

    pairs = [pair(i) for i in range(parts + 1)]
    for load, _ in pairs:
        load.start()
    for load, store in pairs:
        load.wait()
        store.start()
    for _, store in pairs:
        store.wait()


def local(
    query_rows, key_rows, value_rows, gate_rows, log_decay, out_proj,
    moe_input, norm_gain, routing, route_weight,
    expert_gate, expert_up, expert_down, shared_gate, shared_up, shared_down,
):
    E, T = lax.axis_size("ep"), lax.axis_size("tp")
    G = math.gcd(E, Z_GROUPS)
    R = E // G
    Pn = R * T
    B = math.gcd(T, 2)
    A = T // B
    n = query_rows.shape[0]
    H = query_rows.shape[1] // DK
    nb = n // BLOCK
    tok, width = moe_input.shape
    visits = routing.shape[1]
    C = 2 * tok * visits // (E * T)
    ff = expert_gate.shape[2]
    assert shared_gate.shape[1] == ff
    rows_o = n // T
    dvl = H * DV

    vm = pl.BlockSpec(memory_space=pltpu.VMEM)
    hb = pl.BlockSpec(memory_space=pl.ANY)
    V = pltpu.VMEM
    dma = pltpu.SemaphoreType.DMA
    rows_t = H + (-H % 8)
    scratch = [
        V((tok, width), BF16), V((rows_o, width), BF16), V((tok, width), BF16),
        V((nb, H, BLOCK), F32), V((nb, BLOCK, H), F32),
        V((n, H * DK), BF16), V((n, H * DK), BF16), V((n, dvl), BF16), V((n, dvl), BF16),
        V((T,) + out_proj.shape, BF16),
        V((width, ff), BF16), V((width, ff), BF16), V((ff, width), BF16),
        V((G, tok, width), BF16), V((G, 2 * visits, tok), F32),
        V((G, Pn * C, width), BF16), V((G, Pn * C, width), BF16), V((G, Pn * C, width), BF16),
        V((G, tok, Pn * C), BF16), V((tok, width), F32), V((G, tok, width), BF16),
        V((max(nb * H * DK, rows_o * width // DV), DV), F32), V((nb, H, DK, DV), BF16),
        V((R, H, DK, DV), BF16), V((R, rows_t, 128), F32),
        V((G, H, DK, DV), BF16), V((G, rows_t, 128), F32), V((H, DK, DV), F32),
        V((T, rows_o, dvl), BF16), V((T - 1, rows_o, dvl), BF16), V((H, DK, DV), F32),
        dma((12,)), dma((width // DV, 2)), dma,
        dma((2, G)), dma((G,)), dma((2, G)), dma((G,)),
        dma((G,)), dma((G,)), dma((G,)), dma((G,)),
        dma((G,)), dma((G,)),
        dma((R,)), dma((R,)), dma((R,)), dma((R,)), dma((G,)), dma((G,)), dma((G,)), dma((G,)),
        dma((A,)), dma((A,)), dma((A, R)), dma((A, R)), dma((A, B)), dma((A, B)),
        dma((A, 2, G)), dma((A, G)), dma((T, 1)), dma((T, 1)),
    ]
    made = pl.pallas_call(
        functools.partial(kernel, E, T, G, C),
        out_shape=(
            jax.ShapeDtypeStruct((rows_o, width), BF16),
            jax.ShapeDtypeStruct((tok, width), BF16),
        ),
        in_specs=[vm] * 4 + [hb] * 12,
        out_specs=(hb, hb),
        scratch_shapes=scratch,
        compiler_params=pltpu.CompilerParams(
            collective_id=0, has_side_effects=True, vmem_limit_bytes=67043328
        ),
        name="fused",
    )(
        norm_gain[None, :], routing.T, route_weight.T, log_decay,
        moe_input, query_rows, key_rows, value_rows, gate_rows, out_proj,
        expert_gate, expert_up, expert_down, shared_gate, shared_up, shared_down,
    )

    parts = 8
    return pl.pallas_call(
        finish,
        out_shape=tuple(jax.ShapeDtypeStruct(a.shape, a.dtype) for a in made),
        in_specs=[hb] * 2,
        out_specs=(hb, hb),
        scratch_shapes=[V(a.shape, a.dtype) for a in made]
        + [dma((parts + 1,)), dma((parts + 1,))],
        name="finish",
    )(*made)


def solution(mesh):
    both = P(("ep", "tp"), None)
    in_specs = (
        P("ep", "tp"), P("ep", "tp"), P("ep", "tp"), P("ep", "tp"), P("tp", "ep"), P("tp", None),
        both, P(), both, both,
        P(("ep", "tp"), None, None), P(("ep", "tp"), None, None), P(("ep", "tp"), None, None),
        P(), P(), P(),
    )
    return jax.shard_map(
        local, mesh=mesh, in_specs=in_specs, out_specs=(both, both), check_vma=False
    )
```

```python
import functools
import math

import jax
import jax.numpy as jnp
from jax import lax
from jax.experimental import pallas as pl
from jax.experimental.pallas import tpu as pltpu
from jax.sharding import PartitionSpec as P

DK = 128
DV = 256
BLOCK = 128
EPS = 1e-06
Z_GROUPS = 4

F32 = jnp.float32
BF16 = jnp.bfloat16
MESH = pl.DeviceIdType.MESH


def dot(a, b):
    return jnp.dot(a, b, preferred_element_type=F32)


def silu(v):
    return v / (1.0 + jnp.exp(-v))


def kernel(
    E, T, G, C,
    gain_ref, route_ref, rweight_ref, decay_ref,
    x_hbm, q_hbm, k_hbm, v_hbm, g_hbm, op_hbm,
    wg_hbm, wu_hbm, wd_hbm, sg_hbm, su_hbm, sd_hbm,
    mix_hbm, moe_hbm,
    x_v, mix_v, moe_v, cum_ref, cumc_ref,
    q_v, k_v, v_v, g_v, op_v, wg_v, wu_v, wd_v,
    xz, mz, dsp, rcv, ret, dwt, shr, prcv,
    upd, sblk, srcv, trcv, zrcv, pre, rs, rr, inc,
    load_sem, mix_sem, moe_sem,
    z_s, z_r, m_s, m_r, d_s, d_r, b_s, b_r, p_s, p_r, s_s, s_r, t_s, t_r, e_s, e_r,
    o1_s, o1_r, o2_s, o2_r, o3_s, o3_r, oz_s, oz_r, r_s, r_r,
):
    ep = lax.axis_index("ep")
    tp = lax.axis_index("tp")
    R = E // G
    Pn = R * T
    zi = ep // R
    yi = ep % R
    j = yi * T + tp
    tok, width = x_v.shape
    n_visits = route_ref.shape[0]
    nb = cum_ref.shape[0]
    H = cum_ref.shape[1]
    nbc = nb // T
    B = math.gcd(T, 2)
    A = T // B
    ta, tb = tp // B, tp % B
    piece = op_v.shape[1] // E
    scale = DK ** (-0.5)

    loads = [
        pltpu.make_async_copy(src, dst, load_sem.at[i])
        for i, (src, dst) in enumerate(
            ((k_hbm, k_v), (v_hbm, v_v), (op_hbm, op_v.at[tp]), (sg_hbm, wg_v), (su_hbm, wu_v),
             (sd_hbm, wd_v), (q_hbm, q_v), (g_hbm, g_v), (wg_hbm.at[0], wg_v),
             (wu_hbm.at[0], wu_v), (wd_hbm.at[0], wd_v))
        )
    ]
    x_load = pltpu.make_async_copy(x_hbm, x_v, load_sem.at[11])
    x_load.start()
    for c in loads[:8]:
        c.start()

    def z_place(g):
        return (g * R + yi, tp)

    def plane_peer(d):
        p = (j + d) % Pn
        return (zi * R + p // T, p % T)

    barrier = pltpu.get_barrier_semaphore()

    @pl.loop(1, Pn)
    def _(d):
        pl.semaphore_signal(barrier, inc=1, device_id=plane_peer(d), device_id_type=MESH)

    @pl.loop(1, E)
    def _(d):
        pl.semaphore_signal(barrier, inc=1, device_id=((ep + d) % E, tp), device_id_type=MESH)

    x_load.wait()
    xf = x_v[...].astype(F32)
    xz[zi] = (
        xf * lax.rsqrt(jnp.mean(xf * xf, axis=-1, keepdims=True) + EPS) * gain_ref[...]
    ).astype(BF16)
    mz[zi, 0:n_visits] = route_ref[...].astype(F32)
    mz[zi, n_visits:2 * n_visits] = rweight_ref[...]
    pl.semaphore_wait(barrier, Pn - 1 + E - 1)

    def rcopy(src, dst, ss, rs_, dev):
        return pltpu.make_async_remote_copy(
            src_ref=src, dst_ref=dst, send_sem=ss, recv_sem=rs_, device_id=dev, device_id_type=MESH
        )

    def z_copy(g, way):
        to = (zi - 1, zi + 1)[way]
        return rcopy(xz.at[g], xz.at[g], z_s.at[way, g], z_r.at[g], z_place(to))

    def m_copy(g, way):
        to = (zi - 1, zi + 1)[way]
        return rcopy(mz.at[g], mz.at[g], m_s.at[way, g], m_r.at[g], z_place(to))

    def z_sends(g, way):
        if way:
            return (g <= zi) & (zi + 1 < G)
        return (g >= zi) & (zi > 0)

    def nth(n):
        m = jnp.minimum(zi, G - 1 - zi)
        step = (2 * (zi % 2) - 1) * (2 * (n % 2) - 1)
        far = zi + jnp.where(2 * zi > G - 1, m - n, n - m)
        return jnp.where(n <= 2 * m, zi + step * ((n + 1) // 2), far)

    def rows(d):
        return pl.ds(pl.multiple_of(d * C, C), C)

    def d_copy(r, d):
        return rcopy(dsp.at[r, rows(d)], rcv.at[r, rows(d)], d_s.at[r], d_r.at[r], plane_peer(d))

    def b_copy(r, d):
        return rcopy(rcv.at[r, rows(d)], ret.at[r, rows(d)], b_s.at[r], b_r.at[r],
                     plane_peer(Pn - d))

    others = pl.ds(C, (Pn - 1) * C)

    def d_all(r):
        return rcopy(dsp.at[r, others], rcv.at[r, others], d_s.at[r], d_r.at[r], plane_peer(1))

    def b_all(r):
        return rcopy(rcv.at[r, others], ret.at[r, others], b_s.at[r], b_r.at[r], plane_peer(1))

    def p_copy(g):
        return rcopy(dsp.at[g, 0:tok], prcv.at[zi], p_s.at[g], p_r.at[zi], z_place(g))

    def p_arrival(g):
        return rcopy(dsp.at[g, 0:tok], prcv.at[g], p_s.at[g], p_r.at[g], z_place(g))

    def s_copy(d):
        return rcopy(srcv.at[0], srcv.at[d], s_s.at[d], s_r.at[d],
                     (zi * R + (yi + d) % R, tp))

    def t_copy(d):
        return rcopy(trcv.at[0], trcv.at[d], t_s.at[d], t_r.at[d],
                     (zi * R + (yi + d) % R, tp))

    def e_copy():
        return rcopy(zrcv.at[0], zrcv.at[1], e_s, e_r, z_place(zi + 1))

    def shard(da, db=0):
        return ((ta + A - da) % A) * B + (tb + B - db) % B

    def part(y):
        return pl.ds(pl.multiple_of((zi * R + y) * piece, piece), piece)

    def o1_copy(da, src):
        at = op_v.at[src, part(yi)]
        return rcopy(at, at, o1_s.at[da], o1_r.at[da], (ep, ((ta + da) % A) * B + tb))

    def o2_copy(da, dy, y):
        at = op_v.at[shard(da), part(y)]
        return rcopy(at, at, o2_s.at[da, dy], o2_r.at[da, dy], (zi * R + (yi + dy) % R, tp))

    def oz_copy(da, g, way):
        to = (zi - 1, zi + 1)[way]
        at = op_v.at[shard(da), pl.ds(pl.multiple_of(g * R * piece, R * piece), R * piece)]
        return rcopy(at, at, oz_s.at[da, way, g], oz_r.at[da, g], z_place(to))

    def oz_sends(g):
        for da in range(1, A):
            for way in (0, 1):
                @pl.when(z_sends(g, way))
                def _():
                    oz_copy(da, g, way).start()

    def oz_receive(g):
        for da in range(1, A):
            oz_copy(da, g, 0).wait_recv()
        oz_sends(g)

    def o3_copy(da, db, src):
        at = op_v.at[src]
        return rcopy(at, at, o3_s.at[da, db], o3_r.at[da, db], (ep, ta * B + (tb + db) % B))

    halves = 1
    strip = mix_v.shape[0] // halves

    def strip_of(part):
        return slice(part * strip, (part + 1) * strip)

    def r_copy(da, db, part):
        i = da * B + db
        return rcopy(rs.at[i, strip_of(w)], rr.at[i - 1, strip_of(w)],
                     r_s.at[i, part], r_r.at[i, part],
                     (ep, ((ta + da) % A) * B + (tb + db) % B))

    for way in (0, 1):
        @pl.when(z_sends(zi, way))
        def _():
            m_copy(zi, way).start()
            z_copy(zi, way).start()

    def dispatch(r):
        meta = mz[r]
        owner = lax.broadcasted_iota(jnp.int32, (Pn, tok), 0)
        owner = (zi * Pn + (owner + j) % Pn).astype(F32)
        member = jnp.zeros((Pn, tok), F32)
        weight = jnp.zeros((Pn, tok), F32)
        for v in range(n_visits):
            hit = meta[v:v + 1, :] == owner
            member += jnp.where(hit, 1.0, 0.0)
            weight += jnp.where(hit, meta[n_visits + v:n_visits + v + 1, :], 0.0)
        before = lax.broadcasted_iota(jnp.int32, (tok, tok), 0) < lax.broadcasted_iota(
            jnp.int32, (tok, tok), 1
        )
        rank = dot(member.astype(BF16), jnp.where(before, 1.0, 0.0).astype(BF16))
        rank = jnp.where(member > 0.5, rank, -1.0)
        slot = lax.broadcasted_iota(jnp.int32, (C, tok), 0).astype(F32)
        picks, wts = [], []
        for d in range(Pn):
            eq = slot == rank[d:d + 1, :]
            picks.append(jnp.where(eq, 1.0, 0.0))
            wts.append(jnp.where(eq, weight[d:d + 1, :], 0.0))
        pick = jnp.concatenate(picks, axis=0).astype(BF16)
        dwt[r] = jnp.concatenate(wts, axis=0).T.astype(BF16)
        out = dot(pick, xz[r]).astype(BF16)
        dsp[r] = out
        rcv[r, 0:C] = out[0:C]

        @pl.loop(1, Pn)
        def _(d):
            d_copy(r, d).start()

    loads[2].wait()
    for da in range(1, A):
        o1_copy(da, tp).start()

    dispatch(zi)

    blocks = jnp.concatenate(
        [decay_ref[:, b * BLOCK:(b + 1) * BLOCK] for b in range(nb)], axis=0
    )
    upto = lax.broadcasted_iota(jnp.int32, (BLOCK, BLOCK), 0) <= lax.broadcasted_iota(
        jnp.int32, (BLOCK, BLOCK), 1
    )
    cum = jnp.dot(
        blocks, jnp.where(upto, 1.0, 0.0), precision=lax.Precision.HIGHEST,
        preferred_element_type=F32,
    )
    cum_t = cum.T
    for b in range(nb):
        cum_ref[b] = cum[b * H:(b + 1) * H]
        cumc_ref[b] = cum_t[:, b * H:(b + 1) * H]
    trcv[0] = jnp.zeros_like(trcv[0])
    trcv[0, 0:H] = jnp.broadcast_to(
        jnp.sum(decay_ref[...], axis=1, keepdims=True), (H, trcv.shape[2])
    )

    loads[0].wait()
    loads[1].wait()

    def state_rows(b, h):
        return pl.ds(pl.multiple_of((b * H + h) * DK, DK), DK)

    inc[...] = jnp.zeros_like(inc)

    @pl.loop(0, nb)
    def _(b):
        rb = pl.ds(pl.multiple_of(b * BLOCK, BLOCK), BLOCK)
        cumc = cumc_ref[b]
        crow = cum_ref[b]
        for h in range(H):
            col = cumc[:, h:h + 1]
            last = crow[h:h + 1, BLOCK - 1:BLOCK]
            u = (k_v[rb, h * DK:(h + 1) * DK].astype(F32) * (scale * jnp.exp(last - col))).astype(BF16)
            add = lax.dot_general(
                u, v_v[rb, h * DV:(h + 1) * DV], (((0,), (0,)), ((), ())),
                preferred_element_type=F32,
            )
            upd[state_rows(b, h)] = add
            inc[h] = inc[h] * jnp.exp(last) + add

    srcv[0] = inc[...].astype(BF16)

    @pl.loop(1, R)
    def _(d):
        t_copy(d).start()
        s_copy(d).start()

    loads[3].wait()
    loads[4].wait()
    loads[5].wait()
    hid = (silu(dot(xz[zi], wg_v[...])) * dot(xz[zi], wu_v[...])).astype(BF16)
    shr[...] = dot(hid, wd_v[...])
    for c in loads[8:]:
        c.start()

    def give_back(r, wanted):
        @pl.loop(1, Pn)
        def _(d):
            @pl.when(wanted(d))
            def _():
                b_copy(r, d).start()

    def early(d):
        return d % T != T // 2

    def late(d):
        return d % T == T // 2

    def serve(r, *wanted):
        d_all(r).wait_recv()
        rows_in = rcv[r]
        hidden = (silu(dot(rows_in, wg_v[...])) * dot(rows_in, wu_v[...])).astype(BF16)
        res = dot(hidden, wd_v[...]).astype(BF16)
        rcv[r] = res
        ret[r, 0:C] = res[0:C]
        for want in wanted or (early, late):
            give_back(r, want)

    def receive(g):
        m_copy(g, 0).wait_recv()
        z_copy(g, 0).wait_recv()
        for way in (0, 1):
            @pl.when(z_sends(g, way))
            def _():
                m_copy(g, way).start()
                z_copy(g, way).start()

    def plane_state():
        inc[...] = jnp.zeros_like(inc)

        @pl.loop(1, R)
        def _(d):
            t_copy(d).wait_recv()
            s_copy(d).wait_recv()

        @pl.loop(0, R)
        def _(y):
            d = (yi + R - y) % R

            @pl.when(y == yi)
            def _():
                pre[...] = inc[...]

            for h in range(H):
                inc[h] = inc[h] * jnp.exp(trcv[d, h:h + 1, 0:1]) + srcv[d, h].astype(F32)

        zrcv[0] = inc[...].astype(BF16)

        @pl.when((zi == 0) & (zi + 1 < G))
        def _():
            e_copy().start()

    def carry(k):
        @pl.when(zi == k)
        def _():
            e_copy().wait_recv()
            inc[...] = zrcv[1].astype(F32)

            @pl.loop(0, R)
            def _(y):
                for h in range(H):
                    inc[h] = inc[h] * jnp.exp(trcv[y, h:h + 1, 0:1])

            inc[...] += zrcv[0].astype(F32)
            zrcv[0] = inc[...].astype(BF16)
            e_copy().start()

    def carried_state():
        @pl.when(zi == 0)
        def _():
            inc[...] = jnp.zeros_like(inc)

        @pl.when(zi > 0)
        def _():
            @pl.when(zi == G - 1)
            def _():
                e_copy().wait_recv()

            inc[...] = zrcv[1].astype(F32)

        @pl.loop(0, R)
        def _(y):
            @pl.when(y < yi)
            def _():
                for h in range(H):
                    inc[h] = inc[h] * jnp.exp(trcv[(yi + R - y) % R, h:h + 1, 0:1])

        inc[...] += pre[...]

        @pl.loop(0, nb)
        def _(b):
            crow = cum_ref[b]
            for h in range(H):
                s = inc[h]
                sblk[b, h] = s.astype(BF16)
                inc[h] = s * jnp.exp(crow[h:h + 1, BLOCK - 1:BLOCK]) + upd[state_rows(b, h)]

    causal = lax.broadcasted_iota(jnp.int32, (BLOCK, BLOCK), 0) >= lax.broadcasted_iota(
        jnp.int32, (BLOCK, BLOCK), 1
    )

    def retain(i, da, db):
        chunk = ((ta + da) % A) * B + (tb + db) % B

        @pl.loop(0, nbc)
        def _(w):
            b = chunk * nbc + w
            rb = pl.ds(pl.multiple_of(b * BLOCK, BLOCK), BLOCK)
            ro = pl.ds(pl.multiple_of(w * BLOCK, BLOCK), BLOCK)
            cumc = cumc_ref[b]
            crow = cum_ref[b]
            for h in range(H):
                col = cumc[:, h:h + 1]
                row = crow[h:h + 1, :]
                qb = q_v[rb, h * DK:(h + 1) * DK]
                kb = k_v[rb, h * DK:(h + 1) * DK]
                vb = v_v[rb, h * DV:(h + 1) * DV]
                sc = lax.dot_general(qb, kb, (((1,), (1,)), ((), ())), preferred_element_type=F32)
                dec = jnp.exp(jnp.where(causal, col - row, 0.0))
                wt = jnp.where(causal, sc * scale * dec, 0.0).astype(BF16)
                raw = dot(wt, vb) + dot(qb, sblk[b, h]) * jnp.exp(col)
                avg = jnp.mean(raw, axis=-1, keepdims=True)
                cen = raw - avg
                var = jnp.mean(cen * cen, axis=-1, keepdims=True)
                gate = g_v[rb, h * DV:(h + 1) * DV].astype(F32)
                rs[i, ro, h * DV:(h + 1) * DV] = (
                    silu(gate) * (cen * lax.rsqrt(var + EPS))
                ).astype(BF16)

    def combine(r):
        b_all(r).wait_recv()
        d_all(r).wait_send()
        dsp[r, 0:tok] = dot(dwt[r], ret[r]).astype(BF16)
        p_copy(r).start()

    near = [nth(n) for n in range(1, G)]
    for c in loads[8:]:
        c.wait()
    edge = (zi == 0) | (zi == G - 1)
    for da in range(1, A):
        o1_copy(da, shard(da)).wait_recv()
        for dy in range(1, R):
            o2_copy(da, dy, yi).start()
    for db in range(1, B):
        o3_copy(0, db, tp).start()
    receive(near[0])

    @pl.when(jnp.logical_not(edge))
    def _():
        receive(near[1])

    dispatch(near[0])
    plane_state()

    @pl.when(edge)
    def _():
        receive(near[1])

    dispatch(near[1])
    @pl.when(jnp.logical_not(edge))
    def _():
        for g in near[2:]:
            receive(g)
    for da in range(1, A):
        for dy in range(1, R):
            o2_copy(da, dy, (yi + R - dy) % R).wait_recv()
    oz_sends(zi)
    serve(near[0])
    carry(1)
    @pl.when(edge)
    def _():
        for g in near[2:]:
            receive(g)

    for g in near[2:]:
        dispatch(g)
    serve(near[1])
    carry(2)
    oz_receive(near[0])
    combine(near[0])
    serve(zi, early)
    oz_receive(near[1])
    carried_state()
    loads[6].wait()
    loads[7].wait()

    @pl.loop(0, T)
    def _(i):
        retain(i, i // B, i % B)
    for g in near[2:]:
        serve(g)
    @pl.when(jnp.logical_not(edge))
    def _():
        for g in near[2:]:
            oz_receive(g)
    for w in range(halves):
        for da in range(1, A):
            for db in range(B):
                r_copy(da, db, w).start()
        for db in range(1, B):
            r_copy(0, db, w).start()
    give_back(zi, late)
    combine(near[1])
    for g in near[2:]:
        combine(g)
    @pl.when(edge)
    def _():
        for g in near[2:]:
            oz_receive(g)
    for da in range(1, A):
        for db in range(1, B):
            o3_copy(da, db, shard(da)).start()

    for db in range(1, B):
        o3_copy(0, db, shard(0, db)).wait_recv()
        for w in range(halves):
            r_copy(0, db, w).wait_recv()

    n_half = upd.shape[1]
    n_col = 2 * n_half
    n_out = width // n_col

    def columns(n):
        return pl.ds(pl.multiple_of(n * n_col, n_col), n_col)

    def out_rows(n, part):
        return pl.ds(pl.multiple_of((n * 2 + part) * strip, strip), strip)

    @pl.loop(0, n_out)
    def _(n):
        acc = dot(rs[0], op_v[tp, :, columns(n)])
        for db in range(1, B):
            acc += dot(rr[db - 1], op_v[shard(0, db), :, columns(n)])
        for w in range(2):
            upd[out_rows(n, w)] = acc[:, w * n_half:(w + 1) * n_half]

    def mix_out(n, part):
        at = (strip_of(part), columns(n))
        return pltpu.make_async_copy(mix_v.at[at], mix_hbm.at[at], mix_sem.at[n, part])

    for w in range(halves):
        for da in range(1, A):
            for db in range(B):
                if db and not w:
                    o3_copy(da, db, shard(da, db)).wait_recv()
                r_copy(da, db, w).wait_recv()

                @pl.loop(0, n_out)
                def _(n):
                    acc = dot(rr[da * B + db - 1], op_v[shard(da, db), :, columns(n)])
                    for w in range(2):
                        at = slice(w * n_half, (w + 1) * n_half)
                        part_sum = upd[out_rows(n, w)] + acc[:, at]
                        if da == A - 1 and db == B - 1:
                            mix_v[:, pl.ds(pl.multiple_of(n * n_col + w * n_half, n_half), n_half)] = (
                                part_sum.astype(BF16)
                            )
                        else:
                            upd[out_rows(n, w)] = part_sum
                    if da == A - 1 and db == B - 1:
                        mix_out(n, 0).start()

    b_all(zi).wait_recv()
    shr[...] += dot(dwt[zi], ret[zi])
    @pl.loop(1, G)
    def _(i):
        g = (zi + i) % G
        p_arrival(g).wait_recv()
        shr[...] += prcv[g].astype(F32)

    moe_v[...] = shr[...].astype(BF16)
    moe_out = pltpu.make_async_copy(moe_v, moe_hbm, moe_sem)
    moe_out.start()

    @pl.loop(0, G)
    def _(g):
        for way in (0, 1):
            @pl.when(z_sends(g, way))
            def _():
                m_copy(g, way).wait_send()
                z_copy(g, way).wait_send()

        @pl.when(g != zi)
        def _():
            p_copy(g).wait_send()

    @pl.loop(0, G)
    def _(r):
        b_all(r).wait_send()

    d_all(zi).wait_send()

    @pl.loop(1, R)
    def _(d):
        t_copy(d).wait_send()
        s_copy(d).wait_send()

    @pl.when(zi + 1 < G)
    def _():
        e_copy().wait_send()

    for da in range(A):
        for db in range(B):
            if da or db:
                for w in range(halves):
                    r_copy(da, db, w).wait_send()

    for da in range(A):
        if da:
            o1_copy(da, tp).wait_send()
            for dy in range(1, R):
                o2_copy(da, dy, yi).wait_send()
            for g in range(G):
                for way in (0, 1):
                    @pl.when(z_sends(g, way))
                    def _():
                        oz_copy(da, g, way).wait_send()
        for db in range(1, B):
            o3_copy(da, db, shard(da)).wait_send()

    moe_out.wait()

    @pl.loop(0, n_out)
    def _(n):
        for w in range(halves):
            mix_out(n, w).wait()


def finish(mix_in, moe_in, mix_out, moe_out, mix_v, moe_v, in_sem, out_sem):
    parts = in_sem.shape[0] - 1
    strip = mix_v.shape[0] // parts

    def pair(i):
        if i == parts:
            refs = (moe_in, moe_v, moe_out)
        else:
            refs = [r.at[i * strip:(i + 1) * strip] for r in (mix_in, mix_v, mix_out)]
        return (pltpu.make_async_copy(refs[0], refs[1], in_sem.at[i]),
                pltpu.make_async_copy(refs[1], refs[2], out_sem.at[i]))

    pairs = [pair(i) for i in range(parts + 1)]
    for load, _ in pairs:
        load.start()
    for load, store in pairs:
        load.wait()
        store.start()
    for _, store in pairs:
        store.wait()


def local(
    query_rows, key_rows, value_rows, gate_rows, log_decay, out_proj,
    moe_input, norm_gain, routing, route_weight,
    expert_gate, expert_up, expert_down, shared_gate, shared_up, shared_down,
):
    E, T = lax.axis_size("ep"), lax.axis_size("tp")
    G = math.gcd(E, Z_GROUPS)
    R = E // G
    Pn = R * T
    B = math.gcd(T, 2)
    A = T // B
    n = query_rows.shape[0]
    H = query_rows.shape[1] // DK
    nb = n // BLOCK
    tok, width = moe_input.shape
    visits = routing.shape[1]
    C = 2 * tok * visits // (E * T)
    ff = expert_gate.shape[2]
    assert shared_gate.shape[1] == ff
    assert G == Z_GROUPS
    rows_o = n // T
    dvl = H * DV

    vm = pl.BlockSpec(memory_space=pltpu.VMEM)
    hb = pl.BlockSpec(memory_space=pl.ANY)
    V = pltpu.VMEM
    dma = pltpu.SemaphoreType.DMA
    rows_t = H + (-H % 8)
    scratch = [
        V((tok, width), BF16), V((rows_o, width), BF16), V((tok, width), BF16),
        V((nb, H, BLOCK), F32), V((nb, BLOCK, H), F32),
        V((n, H * DK), BF16), V((n, H * DK), BF16), V((n, dvl), BF16), V((n, dvl), BF16),
        V((T,) + out_proj.shape, BF16),
        V((width, ff), BF16), V((width, ff), BF16), V((ff, width), BF16),
        V((G, tok, width), BF16), V((G, 2 * visits, tok), F32),
        V((G, Pn * C, width), BF16), V((G, Pn * C, width), BF16), V((G, Pn * C, width), BF16),
        V((G, tok, Pn * C), BF16), V((tok, width), F32), V((G, tok, width), BF16),
        V((max(nb * H * DK, rows_o * width // DV), DV), F32), V((nb, H, DK, DV), BF16),
        V((R, H, DK, DV), BF16), V((R, rows_t, 128), F32),
        V((2, H, DK, DV), BF16), V((H, DK, DV), F32),
        V((T, rows_o, dvl), BF16), V((T - 1, rows_o, dvl), BF16), V((H, DK, DV), F32),
        dma((12,)), dma((width // DV, 2)), dma,
        dma((2, G)), dma((G,)), dma((2, G)), dma((G,)),
        dma((G,)), dma((G,)), dma((G,)), dma((G,)),
        dma((G,)), dma((G,)),
        dma((R,)), dma((R,)), dma((R,)), dma((R,)), dma, dma,
        dma((A,)), dma((A,)), dma((A, R)), dma((A, R)), dma((A, B)), dma((A, B)),
        dma((A, 2, G)), dma((A, G)), dma((T, 1)), dma((T, 1)),
    ]
    made = pl.pallas_call(
        functools.partial(kernel, E, T, G, C),
        out_shape=(
            jax.ShapeDtypeStruct((rows_o, width), BF16),
            jax.ShapeDtypeStruct((tok, width), BF16),
        ),
        in_specs=[vm] * 4 + [hb] * 12,
        out_specs=(hb, hb),
        scratch_shapes=scratch,
        compiler_params=pltpu.CompilerParams(
            collective_id=0, has_side_effects=True, vmem_limit_bytes=67043328
        ),
        name="fused",
    )(
        norm_gain[None, :], routing.T, route_weight.T, log_decay,
        moe_input, query_rows, key_rows, value_rows, gate_rows, out_proj,
        expert_gate, expert_up, expert_down, shared_gate, shared_up, shared_down,
    )

    parts = 8
    return pl.pallas_call(
        finish,
        out_shape=tuple(jax.ShapeDtypeStruct(a.shape, a.dtype) for a in made),
        in_specs=[hb] * 2,
        out_specs=(hb, hb),
        scratch_shapes=[V(a.shape, a.dtype) for a in made]
        + [dma((parts + 1,)), dma((parts + 1,))],
        name="finish",
    )(*made)


def solution(mesh):
    both = P(("ep", "tp"), None)
    in_specs = (
        P("ep", "tp"), P("ep", "tp"), P("ep", "tp"), P("ep", "tp"), P("tp", "ep"), P("tp", None),
        both, P(), both, both,
        P(("ep", "tp"), None, None), P(("ep", "tp"), None, None), P(("ep", "tp"), None, None),
        P(), P(), P(),
    )
    return jax.shard_map(
        local, mesh=mesh, in_specs=in_specs, out_specs=(both, both), check_vma=False
    )
```

```python
import functools
import math

import jax
import jax.numpy as jnp
from jax import lax
from jax.experimental import pallas as pl
from jax.experimental.pallas import tpu as pltpu
from jax.sharding import PartitionSpec as P

DK = 128
DV = 256
BLOCK = 128
EPS = 1e-06
Z_GROUPS = 4

F32 = jnp.float32
BF16 = jnp.bfloat16
MESH = pl.DeviceIdType.MESH


def dot(a, b):
    return jnp.dot(a, b, preferred_element_type=F32)


def silu(v):
    return v / (1.0 + jnp.exp(-v))


def kernel(
    E, T, G, C,
    gain_ref, route_ref, rweight_ref, decay_ref,
    x_hbm, q_hbm, k_hbm, v_hbm, g_hbm, op_hbm,
    wg_hbm, wu_hbm, wd_hbm, sg_hbm, su_hbm, sd_hbm,
    mix_hbm, moe_hbm,
    x_v, mix_v, moe_v, cum_ref, cumc_ref,
    q_v, k_v, v_v, g_v, op_v, wg_v, wu_v, wd_v,
    xz, mz, dsp, rcv, ret, dwt, shr, prcv,
    upd, sblk, srcv, trcv, zrcv, pre, rs, rr, inc,
    load_sem, mix_sem, moe_sem,
    z_s, z_r, m_s, m_r, d_s, d_r, b_s, b_r, p_s, p_r, s_s, s_r, t_s, t_r, e_s, e_r,
    o1_s, o1_r, o2_s, o2_r, o3_s, o3_r, oz_s, oz_r, r_s, r_r,
):
    ep = lax.axis_index("ep")
    tp = lax.axis_index("tp")
    R = E // G
    Pn = R * T
    zi = ep // R
    yi = ep % R
    j = yi * T + tp
    tok, width = x_v.shape
    n_visits = route_ref.shape[0]
    nb = cum_ref.shape[0]
    H = cum_ref.shape[1]
    nbc = nb // T
    B = math.gcd(T, 2)
    A = T // B
    ta, tb = tp // B, tp % B
    piece = op_v.shape[1] // E
    scale = DK ** (-0.5)

    loads = [
        pltpu.make_async_copy(src, dst, load_sem.at[i])
        for i, (src, dst) in enumerate(
            ((k_hbm, k_v), (v_hbm, v_v), (op_hbm, op_v.at[tp]), (sg_hbm, wg_v), (su_hbm, wu_v),
             (sd_hbm, wd_v), (q_hbm, q_v), (g_hbm, g_v), (wg_hbm.at[0], wg_v),
             (wu_hbm.at[0], wu_v), (wd_hbm.at[0], wd_v))
        )
    ]
    x_load = pltpu.make_async_copy(x_hbm, x_v, load_sem.at[11])
    x_load.start()
    for c in loads[:8]:
        c.start()

    def z_place(g):
        return (g * R + yi, tp)

    def plane_peer(d):
        p = (j + d) % Pn
        return (zi * R + p // T, p % T)

    barrier = pltpu.get_barrier_semaphore()

    @pl.loop(1, Pn)
    def _(d):
        pl.semaphore_signal(barrier, inc=1, device_id=plane_peer(d), device_id_type=MESH)

    @pl.loop(1, E)
    def _(d):
        pl.semaphore_signal(barrier, inc=1, device_id=((ep + d) % E, tp), device_id_type=MESH)

    x_load.wait()
    xf = x_v[...].astype(F32)
    xz[zi] = (
        xf * lax.rsqrt(jnp.mean(xf * xf, axis=-1, keepdims=True) + EPS) * gain_ref[...]
    ).astype(BF16)
    mz[zi, 0:n_visits] = route_ref[...].astype(F32)
    mz[zi, n_visits:2 * n_visits] = rweight_ref[...]
    pl.semaphore_wait(barrier, Pn - 1 + E - 1)

    def rcopy(src, dst, ss, rs_, dev):
        return pltpu.make_async_remote_copy(
            src_ref=src, dst_ref=dst, send_sem=ss, recv_sem=rs_, device_id=dev, device_id_type=MESH
        )

    def z_copy(g, way):
        to = (zi - 1, zi + 1)[way]
        return rcopy(xz.at[g], xz.at[g], z_s.at[way, g], z_r.at[g], z_place(to))

    def m_copy(g, way):
        to = (zi - 1, zi + 1)[way]
        return rcopy(mz.at[g], mz.at[g], m_s.at[way, g], m_r.at[g], z_place(to))

    def z_sends(g, way):
        if way:
            return (g <= zi) & (zi + 1 < G)
        return (g >= zi) & (zi > 0)

    def nth(n):
        m = jnp.minimum(zi, G - 1 - zi)
        step = (2 * (zi % 2) - 1) * (2 * (n % 2) - 1)
        far = zi + jnp.where(2 * zi > G - 1, m - n, n - m)
        return jnp.where(n <= 2 * m, zi + step * ((n + 1) // 2), far)

    def rows(d):
        return pl.ds(pl.multiple_of(d * C, C), C)

    def d_copy(r, d):
        return rcopy(dsp.at[r, rows(d)], rcv.at[r, rows(d)], d_s.at[r], d_r.at[r], plane_peer(d))

    def b_copy(r, d):
        return rcopy(rcv.at[r, rows(d)], ret.at[r, rows(d)], b_s.at[r], b_r.at[r],
                     plane_peer(Pn - d))

    others = pl.ds(C, (Pn - 1) * C)

    def d_all(r):
        return rcopy(dsp.at[r, others], rcv.at[r, others], d_s.at[r], d_r.at[r], plane_peer(1))

    def b_all(r):
        return rcopy(rcv.at[r, others], ret.at[r, others], b_s.at[r], b_r.at[r], plane_peer(1))

    def p_copy(g):
        return rcopy(dsp.at[g, 0:tok], prcv.at[zi], p_s.at[g], p_r.at[zi], z_place(g))

    def p_arrival(g):
        return rcopy(dsp.at[g, 0:tok], prcv.at[g], p_s.at[g], p_r.at[g], z_place(g))

    def s_copy(d):
        return rcopy(srcv.at[0], srcv.at[d], s_s.at[d], s_r.at[d],
                     (zi * R + (yi + d) % R, tp))

    def t_copy(d):
        return rcopy(trcv.at[0], trcv.at[d], t_s.at[d], t_r.at[d],
                     (zi * R + (yi + d) % R, tp))

    def e_copy():
        return rcopy(zrcv.at[0], zrcv.at[1], e_s, e_r, z_place(zi + 1))

    def shard(da, db=0):
        return ((ta + A - da) % A) * B + (tb + B - db) % B

    def part(y):
        return pl.ds(pl.multiple_of((zi * R + y) * piece, piece), piece)

    def o1_copy(da, src):
        at = op_v.at[src, part(yi)]
        return rcopy(at, at, o1_s.at[da], o1_r.at[da], (ep, ((ta + da) % A) * B + tb))

    def o2_copy(da, dy, y):
        at = op_v.at[shard(da), part(y)]
        return rcopy(at, at, o2_s.at[da, dy], o2_r.at[da, dy], (zi * R + (yi + dy) % R, tp))

    def oz_copy(da, g, way):
        to = (zi - 1, zi + 1)[way]
        at = op_v.at[shard(da), pl.ds(pl.multiple_of(g * R * piece, R * piece), R * piece)]
        return rcopy(at, at, oz_s.at[da, way, g], oz_r.at[da, g], z_place(to))

    def oz_sends(g):
        for da in range(1, A):
            for way in (0, 1):
                @pl.when(z_sends(g, way))
                def _():
                    oz_copy(da, g, way).start()

    def oz_receive(g):
        for da in range(1, A):
            oz_copy(da, g, 0).wait_recv()
        oz_sends(g)

    def o3_copy(da, db, src):
        at = op_v.at[src]
        return rcopy(at, at, o3_s.at[da, db], o3_r.at[da, db], (ep, ta * B + (tb + db) % B))

    halves = 1
    strip = mix_v.shape[0] // halves

    def strip_of(part):
        return slice(part * strip, (part + 1) * strip)

    def r_copy(da, db, part):
        i = da * B + db
        return rcopy(rs.at[i, strip_of(w)], rr.at[i - 1, strip_of(w)],
                     r_s.at[i, part], r_r.at[i, part],
                     (ep, ((ta + da) % A) * B + (tb + db) % B))

    for way in (0, 1):
        @pl.when(z_sends(zi, way))
        def _():
            m_copy(zi, way).start()
            z_copy(zi, way).start()

    def dispatch(r):
        meta = mz[r]
        owner = lax.broadcasted_iota(jnp.int32, (Pn, tok), 0)
        owner = (zi * Pn + (owner + j) % Pn).astype(F32)
        member = jnp.zeros((Pn, tok), F32)
        weight = jnp.zeros((Pn, tok), F32)
        for v in range(n_visits):
            hit = meta[v:v + 1, :] == owner
            member += jnp.where(hit, 1.0, 0.0)
            weight += jnp.where(hit, meta[n_visits + v:n_visits + v + 1, :], 0.0)
        before = lax.broadcasted_iota(jnp.int32, (tok, tok), 0) < lax.broadcasted_iota(
            jnp.int32, (tok, tok), 1
        )
        rank = dot(member.astype(BF16), jnp.where(before, 1.0, 0.0).astype(BF16))
        rank = jnp.where(member > 0.5, rank, -1.0)
        slot = lax.broadcasted_iota(jnp.int32, (C, tok), 0).astype(F32)
        picks, wts = [], []
        for d in range(Pn):
            eq = slot == rank[d:d + 1, :]
            picks.append(jnp.where(eq, 1.0, 0.0))
            wts.append(jnp.where(eq, weight[d:d + 1, :], 0.0))
        pick = jnp.concatenate(picks, axis=0).astype(BF16)
        dwt[r] = jnp.concatenate(wts, axis=0).T.astype(BF16)
        out = dot(pick, xz[r]).astype(BF16)
        dsp[r] = out
        rcv[r, 0:C] = out[0:C]

        @pl.loop(1, Pn)
        def _(d):
            d_copy(r, d).start()

    loads[2].wait()
    for da in range(1, A):
        o1_copy(da, tp).start()

    dispatch(zi)

    blocks = jnp.concatenate(
        [decay_ref[:, b * BLOCK:(b + 1) * BLOCK] for b in range(nb)], axis=0
    )
    upto = lax.broadcasted_iota(jnp.int32, (BLOCK, BLOCK), 0) <= lax.broadcasted_iota(
        jnp.int32, (BLOCK, BLOCK), 1
    )
    cum = jnp.dot(
        blocks, jnp.where(upto, 1.0, 0.0), precision=lax.Precision.HIGHEST,
        preferred_element_type=F32,
    )
    cum_t = cum.T
    for b in range(nb):
        cum_ref[b] = cum[b * H:(b + 1) * H]
        cumc_ref[b] = cum_t[:, b * H:(b + 1) * H]
    trcv[0] = jnp.zeros_like(trcv[0])
    trcv[0, 0:H] = jnp.broadcast_to(
        jnp.sum(decay_ref[...], axis=1, keepdims=True), (H, trcv.shape[2])
    )

    loads[0].wait()
    loads[1].wait()

    def state_rows(b, h):
        return pl.ds(pl.multiple_of((b * H + h) * DK, DK), DK)

    inc[...] = jnp.zeros_like(inc)

    @pl.loop(0, nb)
    def _(b):
        rb = pl.ds(pl.multiple_of(b * BLOCK, BLOCK), BLOCK)
        cumc = cumc_ref[b]
        crow = cum_ref[b]
        for h in range(H):
            col = cumc[:, h:h + 1]
            last = crow[h:h + 1, BLOCK - 1:BLOCK]
            u = (k_v[rb, h * DK:(h + 1) * DK].astype(F32) * (scale * jnp.exp(last - col))).astype(BF16)
            add = lax.dot_general(
                u, v_v[rb, h * DV:(h + 1) * DV], (((0,), (0,)), ((), ())),
                preferred_element_type=F32,
            )
            upd[state_rows(b, h)] = add
            inc[h] = inc[h] * jnp.exp(last) + add

    srcv[0] = inc[...].astype(BF16)

    @pl.loop(1, R)
    def _(d):
        t_copy(d).start()
        s_copy(d).start()

    loads[3].wait()
    loads[4].wait()
    loads[5].wait()
    hid = (silu(dot(xz[zi], wg_v[...])) * dot(xz[zi], wu_v[...])).astype(BF16)
    shr[...] = dot(hid, wd_v[...])
    for c in loads[8:]:
        c.start()

    def give_back(r, wanted):
        @pl.loop(1, Pn)
        def _(d):
            @pl.when(wanted(d))
            def _():
                b_copy(r, d).start()

    def early(d):
        return d % T != T // 2

    def late(d):
        return d % T == T // 2

    def serve(r, *wanted):
        d_all(r).wait_recv()
        rows_in = rcv[r]
        hidden = (silu(dot(rows_in, wg_v[...])) * dot(rows_in, wu_v[...])).astype(BF16)
        res = dot(hidden, wd_v[...]).astype(BF16)
        rcv[r] = res
        ret[r, 0:C] = res[0:C]
        for want in wanted or (early, late):
            give_back(r, want)

    def receive(g):
        m_copy(g, 0).wait_recv()
        z_copy(g, 0).wait_recv()
        for way in (0, 1):
            @pl.when(z_sends(g, way))
            def _():
                m_copy(g, way).start()
                z_copy(g, way).start()

    def plane_state():
        inc[...] = jnp.zeros_like(inc)

        @pl.loop(1, R)
        def _(d):
            t_copy(d).wait_recv()
            s_copy(d).wait_recv()

        @pl.loop(0, R)
        def _(y):
            d = (yi + R - y) % R

            @pl.when(y == yi)
            def _():
                pre[...] = inc[...]

            for h in range(H):
                inc[h] = inc[h] * jnp.exp(trcv[d, h:h + 1, 0:1]) + srcv[d, h].astype(F32)

        zrcv[0] = inc[...].astype(BF16)

        @pl.when((zi == 0) & (zi + 1 < G))
        def _():
            e_copy().start()

    def carry(k):
        @pl.when(zi == k)
        def _():
            e_copy().wait_recv()
            inc[...] = zrcv[1].astype(F32)

            @pl.loop(0, R)
            def _(y):
                for h in range(H):
                    inc[h] = inc[h] * jnp.exp(trcv[y, h:h + 1, 0:1])

            inc[...] += zrcv[0].astype(F32)
            zrcv[0] = inc[...].astype(BF16)
            e_copy().start()

    def carried_state():
        @pl.when(zi == 0)
        def _():
            inc[...] = jnp.zeros_like(inc)

        @pl.when(zi > 0)
        def _():
            @pl.when(zi == G - 1)
            def _():
                e_copy().wait_recv()

            inc[...] = zrcv[1].astype(F32)

        @pl.loop(0, R)
        def _(y):
            @pl.when(y < yi)
            def _():
                for h in range(H):
                    inc[h] = inc[h] * jnp.exp(trcv[(yi + R - y) % R, h:h + 1, 0:1])

        inc[...] += pre[...]

        @pl.loop(0, nb)
        def _(b):
            crow = cum_ref[b]
            for h in range(H):
                s = inc[h]
                sblk[b, h] = s.astype(BF16)
                inc[h] = s * jnp.exp(crow[h:h + 1, BLOCK - 1:BLOCK]) + upd[state_rows(b, h)]

    causal = lax.broadcasted_iota(jnp.int32, (BLOCK, BLOCK), 0) >= lax.broadcasted_iota(
        jnp.int32, (BLOCK, BLOCK), 1
    )

    def retain(i, da, db):
        chunk = ((ta + da) % A) * B + (tb + db) % B

        @pl.loop(0, nbc)
        def _(w):
            b = chunk * nbc + w
            rb = pl.ds(pl.multiple_of(b * BLOCK, BLOCK), BLOCK)
            ro = pl.ds(pl.multiple_of(w * BLOCK, BLOCK), BLOCK)
            cumc = cumc_ref[b]
            crow = cum_ref[b]
            for h in range(H):
                col = cumc[:, h:h + 1]
                row = crow[h:h + 1, :]
                qb = q_v[rb, h * DK:(h + 1) * DK]
                kb = k_v[rb, h * DK:(h + 1) * DK]
                vb = v_v[rb, h * DV:(h + 1) * DV]
                sc = lax.dot_general(qb, kb, (((1,), (1,)), ((), ())), preferred_element_type=F32)
                dec = jnp.exp(jnp.where(causal, col - row, 0.0))
                wt = jnp.where(causal, sc * scale * dec, 0.0).astype(BF16)
                raw = dot(wt, vb) + dot(qb, sblk[b, h]) * jnp.exp(col)
                avg = jnp.mean(raw, axis=-1, keepdims=True)
                cen = raw - avg
                var = jnp.mean(cen * cen, axis=-1, keepdims=True)
                gate = g_v[rb, h * DV:(h + 1) * DV].astype(F32)
                rs[i, ro, h * DV:(h + 1) * DV] = (
                    silu(gate) * (cen * lax.rsqrt(var + EPS))
                ).astype(BF16)

    def combine(r):
        b_all(r).wait_recv()
        d_all(r).wait_send()
        dsp[r, 0:tok] = dot(dwt[r], ret[r]).astype(BF16)
        p_copy(r).start()

    near = [nth(n) for n in range(1, G)]
    for c in loads[8:]:
        c.wait()
    edge = (zi == 0) | (zi == G - 1)
    for da in range(1, A):
        o1_copy(da, shard(da)).wait_recv()
        for dy in range(1, R):
            o2_copy(da, dy, yi).start()
    for db in range(1, B):
        o3_copy(0, db, tp).start()
    receive(near[0])

    @pl.when(jnp.logical_not(edge))
    def _():
        receive(near[1])

    dispatch(near[0])
    plane_state()

    @pl.when(edge)
    def _():
        receive(near[1])

    dispatch(near[1])
    @pl.when(jnp.logical_not(edge))
    def _():
        for g in near[2:]:
            receive(g)
    for da in range(1, A):
        for dy in range(1, R):
            o2_copy(da, dy, (yi + R - dy) % R).wait_recv()
    oz_sends(zi)
    serve(near[0])
    carry(1)
    @pl.when(edge)
    def _():
        for g in near[2:]:
            receive(g)

    for g in near[2:]:
        dispatch(g)
    serve(near[1])
    carry(2)
    oz_receive(near[0])
    combine(near[0])
    oz_receive(near[1])
    carried_state()
    loads[6].wait()
    loads[7].wait()

    @pl.loop(0, T)
    def _(i):
        retain(i, i // B, i % B)
    serve(zi, early)
    for g in near[2:]:
        serve(g)
    @pl.when(jnp.logical_not(edge))
    def _():
        for g in near[2:]:
            oz_receive(g)
    combine(near[1])
    for w in range(halves):
        for da in range(1, A):
            for db in range(B):
                r_copy(da, db, w).start()
        for db in range(1, B):
            r_copy(0, db, w).start()
    give_back(zi, late)
    for g in near[2:]:
        combine(g)
    @pl.when(edge)
    def _():
        for g in near[2:]:
            oz_receive(g)
    for da in range(1, A):
        for db in range(1, B):
            o3_copy(da, db, shard(da)).start()

    for db in range(1, B):
        o3_copy(0, db, shard(0, db)).wait_recv()
        for w in range(halves):
            r_copy(0, db, w).wait_recv()

    n_half = upd.shape[1]
    n_col = 2 * n_half
    n_out = width // n_col

    def columns(n):
        return pl.ds(pl.multiple_of(n * n_col, n_col), n_col)

    def out_rows(n, part):
        return pl.ds(pl.multiple_of((n * 2 + part) * strip, strip), strip)

    @pl.loop(0, n_out)
    def _(n):
        acc = dot(rs[0], op_v[tp, :, columns(n)])
        for db in range(1, B):
            acc += dot(rr[db - 1], op_v[shard(0, db), :, columns(n)])
        for w in range(2):
            upd[out_rows(n, w)] = acc[:, w * n_half:(w + 1) * n_half]

    def mix_out(n, part):
        at = (strip_of(part), columns(n))
        return pltpu.make_async_copy(mix_v.at[at], mix_hbm.at[at], mix_sem.at[n, part])

    for w in range(halves):
        for da in range(1, A):
            for db in range(B):
                if db and not w:
                    o3_copy(da, db, shard(da, db)).wait_recv()
                r_copy(da, db, w).wait_recv()

                @pl.loop(0, n_out)
                def _(n):
                    acc = dot(rr[da * B + db - 1], op_v[shard(da, db), :, columns(n)])
                    for w in range(2):
                        at = slice(w * n_half, (w + 1) * n_half)
                        part_sum = upd[out_rows(n, w)] + acc[:, at]
                        if da == A - 1 and db == B - 1:
                            mix_v[:, pl.ds(pl.multiple_of(n * n_col + w * n_half, n_half), n_half)] = (
                                part_sum.astype(BF16)
                            )
                        else:
                            upd[out_rows(n, w)] = part_sum
                    if da == A - 1 and db == B - 1:
                        mix_out(n, 0).start()

    b_all(zi).wait_recv()
    shr[...] += dot(dwt[zi], ret[zi])
    @pl.loop(1, G)
    def _(i):
        g = (zi + i) % G
        p_arrival(g).wait_recv()
        shr[...] += prcv[g].astype(F32)

    moe_v[...] = shr[...].astype(BF16)
    moe_out = pltpu.make_async_copy(moe_v, moe_hbm, moe_sem)
    moe_out.start()

    @pl.loop(0, G)
    def _(g):
        for way in (0, 1):
            @pl.when(z_sends(g, way))
            def _():
                m_copy(g, way).wait_send()
                z_copy(g, way).wait_send()

        @pl.when(g != zi)
        def _():
            p_copy(g).wait_send()

    @pl.loop(0, G)
    def _(r):
        b_all(r).wait_send()

    d_all(zi).wait_send()

    @pl.loop(1, R)
    def _(d):
        t_copy(d).wait_send()
        s_copy(d).wait_send()

    @pl.when(zi + 1 < G)
    def _():
        e_copy().wait_send()

    for da in range(A):
        for db in range(B):
            if da or db:
                for w in range(halves):
                    r_copy(da, db, w).wait_send()

    for da in range(A):
        if da:
            o1_copy(da, tp).wait_send()
            for dy in range(1, R):
                o2_copy(da, dy, yi).wait_send()
            for g in range(G):
                for way in (0, 1):
                    @pl.when(z_sends(g, way))
                    def _():
                        oz_copy(da, g, way).wait_send()
        for db in range(1, B):
            o3_copy(da, db, shard(da)).wait_send()

    moe_out.wait()

    @pl.loop(0, n_out)
    def _(n):
        for w in range(halves):
            mix_out(n, w).wait()


def finish(mix_in, moe_in, mix_out, moe_out, mix_v, moe_v, in_sem, out_sem):
    parts = in_sem.shape[0] - 1
    strip = mix_v.shape[0] // parts

    def pair(i):
        if i == parts:
            refs = (moe_in, moe_v, moe_out)
        else:
            refs = [r.at[i * strip:(i + 1) * strip] for r in (mix_in, mix_v, mix_out)]
        return (pltpu.make_async_copy(refs[0], refs[1], in_sem.at[i]),
                pltpu.make_async_copy(refs[1], refs[2], out_sem.at[i]))

    pairs = [pair(i) for i in range(parts + 1)]
    for load, _ in pairs:
        load.start()
    for load, store in pairs:
        load.wait()
        store.start()
    for _, store in pairs:
        store.wait()


def local(
    query_rows, key_rows, value_rows, gate_rows, log_decay, out_proj,
    moe_input, norm_gain, routing, route_weight,
    expert_gate, expert_up, expert_down, shared_gate, shared_up, shared_down,
):
    E, T = lax.axis_size("ep"), lax.axis_size("tp")
    G = math.gcd(E, Z_GROUPS)
    R = E // G
    Pn = R * T
    B = math.gcd(T, 2)
    A = T // B
    n = query_rows.shape[0]
    H = query_rows.shape[1] // DK
    nb = n // BLOCK
    tok, width = moe_input.shape
    visits = routing.shape[1]
    C = 2 * tok * visits // (E * T)
    ff = expert_gate.shape[2]
    assert shared_gate.shape[1] == ff
    assert G == Z_GROUPS
    rows_o = n // T
    dvl = H * DV

    vm = pl.BlockSpec(memory_space=pltpu.VMEM)
    hb = pl.BlockSpec(memory_space=pl.ANY)
    V = pltpu.VMEM
    dma = pltpu.SemaphoreType.DMA
    rows_t = H + (-H % 8)
    scratch = [
        V((tok, width), BF16), V((rows_o, width), BF16), V((tok, width), BF16),
        V((nb, H, BLOCK), F32), V((nb, BLOCK, H), F32),
        V((n, H * DK), BF16), V((n, H * DK), BF16), V((n, dvl), BF16), V((n, dvl), BF16),
        V((T,) + out_proj.shape, BF16),
        V((width, ff), BF16), V((width, ff), BF16), V((ff, width), BF16),
        V((G, tok, width), BF16), V((G, 2 * visits, tok), F32),
        V((G, Pn * C, width), BF16), V((G, Pn * C, width), BF16), V((G, Pn * C, width), BF16),
        V((G, tok, Pn * C), BF16), V((tok, width), F32), V((G, tok, width), BF16),
        V((max(nb * H * DK, rows_o * width // DV), DV), F32), V((nb, H, DK, DV), BF16),
        V((R, H, DK, DV), BF16), V((R, rows_t, 128), F32),
        V((2, H, DK, DV), BF16), V((H, DK, DV), F32),
        V((T, rows_o, dvl), BF16), V((T - 1, rows_o, dvl), BF16), V((H, DK, DV), F32),
        dma((12,)), dma((width // DV, 2)), dma,
        dma((2, G)), dma((G,)), dma((2, G)), dma((G,)),
        dma((G,)), dma((G,)), dma((G,)), dma((G,)),
        dma((G,)), dma((G,)),
        dma((R,)), dma((R,)), dma((R,)), dma((R,)), dma, dma,
        dma((A,)), dma((A,)), dma((A, R)), dma((A, R)), dma((A, B)), dma((A, B)),
        dma((A, 2, G)), dma((A, G)), dma((T, 1)), dma((T, 1)),
    ]
    made = pl.pallas_call(
        functools.partial(kernel, E, T, G, C),
        out_shape=(
            jax.ShapeDtypeStruct((rows_o, width), BF16),
            jax.ShapeDtypeStruct((tok, width), BF16),
        ),
        in_specs=[vm] * 4 + [hb] * 12,
        out_specs=(hb, hb),
        scratch_shapes=scratch,
        compiler_params=pltpu.CompilerParams(
            collective_id=0, has_side_effects=True, vmem_limit_bytes=67043328
        ),
        name="fused",
    )(
        norm_gain[None, :], routing.T, route_weight.T, log_decay,
        moe_input, query_rows, key_rows, value_rows, gate_rows, out_proj,
        expert_gate, expert_up, expert_down, shared_gate, shared_up, shared_down,
    )

    parts = 8
    return pl.pallas_call(
        finish,
        out_shape=tuple(jax.ShapeDtypeStruct(a.shape, a.dtype) for a in made),
        in_specs=[hb] * 2,
        out_specs=(hb, hb),
        scratch_shapes=[V(a.shape, a.dtype) for a in made]
        + [dma((parts + 1,)), dma((parts + 1,))],
        name="finish",
    )(*made)


def solution(mesh):
    both = P(("ep", "tp"), None)
    in_specs = (
        P("ep", "tp"), P("ep", "tp"), P("ep", "tp"), P("ep", "tp"), P("tp", "ep"), P("tp", None),
        both, P(), both, both,
        P(("ep", "tp"), None, None), P(("ep", "tp"), None, None), P(("ep", "tp"), None, None),
        P(), P(), P(),
    )
    return jax.shard_map(
        local, mesh=mesh, in_specs=in_specs, out_specs=(both, both), check_vma=False
    )
```
